512 devices in a mesh: ep: 32 (over z, core), tp: 16 (over y, x).
Axes of the slice: x: 4, y: 4, z: 16, core: 2. Of those that a mesh axis runs over, the one named last changes fastest.
Arguments:
- tokens: bfloat16 [1536, 2048], P('ep'), may hold values from -6 to 6
- retention_state: float32 [1536, 16, 64, 64], P('ep', 'tp'), may hold values from -1.5 to 1.5
- lengths: int32 [1536], P('ep'), may hold values from 1024 to 16383
- query_weight: bfloat16 [2048, 1024], P(None, 'tp'), may hold values from -0.125 to 0.125
- key_weight: bfloat16 [2048, 1024], P(None, 'tp'), may hold values from -0.125 to 0.125
- value_weight: bfloat16 [2048, 1024], P(None, 'tp'), may hold values from -0.125 to 0.125
- gate_weight: bfloat16 [2048, 1024], P(None, 'tp'), may hold values from -0.125 to 0.125
- out_weight: bfloat16 [1024, 2048], P(None, 'tp'), may hold values from -0.1875 to 0.1875
- first_gain: float32 [2048], replicated, may hold values from 0.1 to 1.9
- routing: int32 [1536, 4], P('ep'), may hold values from 0 to 127, all different within a row; in each aligned block of 48 rows (0 to 47, 48 to 95, ...) at most 5 rows name the same one
- route_weight: float32 [1536, 4], P('ep'), may hold values from 0.1 to 1
- expert_gate: bfloat16 [128, 2048, 512], P('ep', None, 'tp'), may hold values from -0.125 to 0.125
- expert_up: bfloat16 [128, 2048, 512], P('ep', None, 'tp'), may hold values from -0.125 to 0.125
- expert_down: bfloat16 [128, 512, 2048], P('ep', None, 'tp'), may hold values from -0.25 to 0.25
- shared_gate: bfloat16 [2048, 512], P(None, 'tp'), may hold values from -0.125 to 0.125
- shared_up: bfloat16 [2048, 512], P(None, 'tp'), may hold values from -0.125 to 0.125
- shared_down: bfloat16 [512, 2048], P(None, 'tp'), may hold values from -0.25 to 0.25
- side_gate: bfloat16 [2048, 256], P('ep', 'tp'), may hold values from -0.125 to 0.125
- side_up: bfloat16 [2048, 256], P('ep', 'tp'), may hold values from -0.125 to 0.125
- side_down: bfloat16 [256, 2048], P(None, 'tp'), may hold values from -0.375 to 0.375
- side_switch: bfloat16 [2048], replicated, may hold values from -0.125 to 0.125
- second_gain: float32 [2048], P('tp'), may hold values from 0.1 to 1.9
Outputs:
- output: bfloat16 [1536, 2048], P('ep', 'tp')
- new_state: float32 [1536, 16, 64, 64], P('ep', 'tp')
The draws below stay inside these ranges and needn't reach their ends.
Inputs may be any that keep to these rules, and one draw needn't show every extreme that they name: `routing`: each row names 4 different experts. Among the rows of one ep index (aligned blocks of 48 rows) no expert is named by more than 5 rows, a bound that some block reaches.
All inputs are finite; a program needn't handle non-finite values.
Results may differ from the reference program's by a relative error of at most 0.013.
Values may be sent and summed in bfloat16 or wider, within the bound.
No kernel may reach another device: no remote copies, remote signals or barrier semaphores. Data moves between devices by JAX's collectives and lax.ppermute only.
A program may use at most 64 MiB of HBM per device.

```python
import math
import jax
import jax.numpy as jnp
import numpy as np
from jax import lax

D = 2048
HEADS = 16
HEAD_SIZE = 64
FE = 512
SHARED_F = 512
DENSE_F = 256
TOPK = 4
SEQ_DEV = 48
BATCH = 1536
EXPERTS = 128
CAP = 5
N_EP = 32


def touch_ends(array, own_key, low, largest):
    longest = array.shape.index(max(array.shape))
    spots = []
    for shift in (0, 1):
        where = [jax.random.randint(jax.random.fold_in(own_key, axis), (), 0, length) for axis, length in enumerate(array.shape)]
        where[longest] = (where[longest] + shift) % array.shape[longest]
        spots.append(tuple(where))
    return array.at[spots[0]].set(low).at[spots[1]].set(largest)


def levels(rng, extent, cuts, low, largest):
    level, own = 1.0, jax.random.fold_in(rng, 6)
    for dim, shards_of in cuts:
        steps = jnp.exp(jax.random.uniform(jax.random.fold_in(own, dim), (shards_of,), jnp.float32, low / len(cuts), largest / len(cuts)))
        level = level * jnp.repeat(steps, extent[dim] // shards_of).reshape([-1 if axis == dim else 1 for axis in range(len(extent))])
    return level


def assign_block(key, own, number, rows, number_of, top, bound, slope):
    ranking = jax.random.permutation(key, number_of)
    crowded, ordinary = portions_of(number_of, rows * top, bound, slope, True), portions_of(number_of, rows * top, bound, slope, False)
    places = jnp.arange(number_of)

    def named(sizes, offset_by):
        used = int((sizes > 0).sum())
        fixed = max(1, used // 4)
        shifted = fixed + (places - fixed + offset_by * (used - fixed)) % max(1, number_of - fixed)
        return jnp.zeros((number_of,), jnp.int32).at[ranking[jnp.where(places < fixed, places, shifted)]].set(jnp.asarray(sizes, jnp.int32))

    sizes = jnp.where(number % 4 == 0, named(crowded, number // 4), named(ordinary, number - number // 4 - 1))
    mixed = jax.random.permutation(jax.random.fold_in(own, 3), number_of)
    giver, receiver = mixed[0:number_of // 2 * 2:2], mixed[1:number_of // 2 * 2:2]
    room = jnp.minimum(sizes[giver] - 1, bound - sizes[receiver]) // 2
    room = jnp.where((giver == ranking[0]) | (receiver == ranking[0]) | (sizes[receiver] == 0), 0, jnp.maximum(room, 0))
    shifted = jax.random.randint(jax.random.fold_in(own, 4), (number_of // 2,), 0, 1 << 20) % (room + 1)
    sizes = sizes.at[giver].add(-shifted).at[receiver].add(shifted)
    items = jnp.searchsorted(jnp.cumsum(sizes), jnp.arange(rows * top), side="right").astype(jnp.int32)
    listing = items.reshape(top, rows).T
    listing = listing[jax.random.permutation(jax.random.fold_in(own, 1), rows)]
    offset_by = jax.random.randint(jax.random.fold_in(own, 2), (rows, 1), 0, top)
    return jnp.take_along_axis(listing, (jnp.arange(top)[None, :] + offset_by) % top, axis=1)


def portions_of(count, total, most, lean, full):
    weights = [(1 << 20) // math.isqrt(standing ** lean) + 1 for standing in range(1, count + 1)]
    largest = most if full else min(most, max(-(-total // count), total * weights[0] // sum(weights)))
    least = 1 if total - largest >= count - 1 else 0
    given, rest = [largest] + [least] * (count - 1), total - largest - least * (count - 1)
    while rest > 0:
        movable = [i for i in range(1, count) if given[i] < largest] or [i for i in range(1, count) if given[i] < most]
        whole, left = sum([weights[i] for i in movable]), rest
        for i in movable:
            addition = min(most - given[i], max(1, left * weights[i] // whole), rest)
            given[i] = given[i] + addition
            rest = rest - addition
    return np.array(given)


def bell_draw(stream_key, shape, deviation, bound, shards=(), kind=jnp.bfloat16):
    array = jax.random.normal(stream_key, shape, jnp.float32) * deviation
    if len(shards) > 0:
        array = levels(stream_key, shape, shards, -0.22, 0.18) * array
    return jnp.clip(array, min=-bound, max=bound).astype(kind)


def setup_inputs(seed: int = 0) -> dict:
    key_list = jax.random.split(jax.random.key(seed), 23)
    tokens = bell_draw(key_list[0], (BATCH, D), 1.0, 6.0, ((0, 32),))
    retention_state = bell_draw(key_list[1], (BATCH, HEADS, HEAD_SIZE, HEAD_SIZE), 0.25, 1.5, ((0, 32), (1, 16)), jnp.float32)
    lengths = touch_ends(jax.random.randint(key_list[2], (BATCH,), 1024, 16384), jax.random.fold_in(key_list[2], 1), 1024, 16383).astype(jnp.int32)
    query_weight = bell_draw(key_list[3], (D, HEADS * HEAD_SIZE), D ** -0.5, 0.125, ((1, 16),))
    key_weight = bell_draw(key_list[4], (D, HEADS * HEAD_SIZE), D ** -0.5, 0.125, ((1, 16),))
    value_weight = bell_draw(key_list[5], (D, HEADS * HEAD_SIZE), D ** -0.5, 0.125, ((1, 16),))
    gate_weight = bell_draw(key_list[6], (D, HEADS * HEAD_SIZE), D ** -0.5, 0.125, ((1, 16),))
    out_weight = bell_draw(key_list[7], (HEADS * HEAD_SIZE, D), (HEADS * HEAD_SIZE) ** -0.5, 0.1875, ((1, 16),))
    first_gain = jnp.clip(1.0 + 0.18 * jax.random.normal(key_list[8], (D,), jnp.float32), 0.1, 1.9)
    routing_keys = jax.random.split(jax.random.fold_in(key_list[9], 1), BATCH // SEQ_DEV)
    routing_turns = jax.random.permutation(jax.random.fold_in(key_list[9], 3), BATCH // SEQ_DEV)
    routing = jax.vmap(lambda own, number: assign_block(jax.random.fold_in(key_list[9], 2), own, number, SEQ_DEV, EXPERTS, TOPK, CAP, 2))(routing_keys, routing_turns).reshape((BATCH, TOPK))
    route_weight = jnp.clip(0.1 + 0.9 * jax.random.uniform(key_list[10], (BATCH, TOPK), jnp.float32) ** levels(key_list[10], (BATCH, TOPK), ((0, 32),), -0.2, 0.2), 0.1, 1.0)
    expert_gate = bell_draw(key_list[11], (EXPERTS, D, FE), D ** -0.5, 0.125, ((0, 32), (2, 16)))
    expert_up = bell_draw(key_list[12], (EXPERTS, D, FE), D ** -0.5, 0.125, ((0, 32), (2, 16)))
    expert_down = bell_draw(key_list[13], (EXPERTS, FE, D), FE ** -0.5, 0.25, ((0, 32), (2, 16)))
    shared_gate = bell_draw(key_list[14], (D, SHARED_F), D ** -0.5, 0.125, ((1, 16),))
    shared_up = bell_draw(key_list[15], (D, SHARED_F), D ** -0.5, 0.125, ((1, 16),))
    shared_down = bell_draw(key_list[16], (SHARED_F, D), SHARED_F ** -0.5, 0.25, ((1, 16),))
    side_gate = bell_draw(key_list[17], (D, DENSE_F), D ** -0.5, 0.125, ((0, 32), (1, 16)))
    side_up = bell_draw(key_list[18], (D, DENSE_F), D ** -0.5, 0.125, ((0, 32), (1, 16)))
    side_down = bell_draw(key_list[19], (DENSE_F, D), DENSE_F ** -0.5, 0.375, ((1, 16),))
    side_switch = bell_draw(key_list[20], (D,), D ** -0.5, 0.125)
    second_gain = jnp.clip(1.0 + 0.18 * jax.random.normal(key_list[21], (D,), jnp.float32), 0.1, 1.9)
    return {"tokens": tokens, "retention_state": retention_state, "lengths": lengths, "query_weight": query_weight, "key_weight": key_weight, "value_weight": value_weight, "gate_weight": gate_weight, "out_weight": out_weight, "first_gain": first_gain, "routing": routing, "route_weight": route_weight, "expert_gate": expert_gate, "expert_up": expert_up, "expert_down": expert_down, "shared_gate": shared_gate, "shared_up": shared_up, "shared_down": shared_down, "side_gate": side_gate, "side_up": side_up, "side_down": side_down, "side_switch": side_switch, "second_gain": second_gain}


RESIDUAL_SCALE = 2.0 ** 0.25
NORM_EPS = 1e-05
GROUP_EPS = 1e-06
ROPE_BASE = 10000.0

def rotate(vector, positions):
    half_width = vector.shape[-1] // 2
    frequency = ROPE_BASE ** (-jnp.arange(half_width, dtype=jnp.float32) / half_width)
    angles = positions.astype(jnp.float32)[:, None, None] * frequency[None, None, :]
    cosine = jnp.cos(angles)
    sine_part = jnp.sin(angles)
    first_half = vector[..., :half_width]
    second_half = vector[..., half_width:]
    return jnp.concatenate([first_half * cosine - second_half * sine_part, second_half * cosine + first_half * sine_part], -1)

def retain(tokens, retention_state, lengths, query_weight, key_weight, value_weight, gate_weight, first_head):
    row_count = tokens.shape[0]
    head_count = retention_state.shape[1]
    head_width = retention_state.shape[2]

    def project(weight):
        rounded = jnp.dot(tokens, weight, preferred_element_type=jnp.float32).astype(jnp.bfloat16)
        return lax.optimization_barrier(rounded).astype(jnp.float32)
    queries = rotate(project(query_weight).reshape(row_count, head_count, head_width), lengths)
    key_rows = rotate(project(key_weight).reshape(row_count, head_count, head_width), lengths) * head_width ** (-0.5)
    values = project(value_weight).reshape(row_count, head_count, head_width)
    gate_act = project(gate_weight)
    head_index = (first_head + jnp.arange(head_count)).astype(jnp.float32)
    decays = 1.0 - 2.0 ** (-5.0 - 7.0 * head_index / (HEADS - 1))
    own_term = lax.optimization_barrier(jnp.sum(queries * key_rows, -1, keepdims=True)) * values
    carried = decays[None, :, None] * jnp.einsum('bhd,bhde->bhe', queries, retention_state, precision=lax.Precision.HIGHEST)
    result = own_term + carried
    new_state = decays[None, :, None, None] * retention_state + key_rows[:, :, :, None] * values[:, :, None, :]
    normed = result * lax.rsqrt(lax.optimization_barrier(jnp.mean(result * result, -1, keepdims=True)) + GROUP_EPS)
    mixed_heads = (normed.reshape(row_count, head_count * head_width) * jax.nn.silu(gate_act)).astype(jnp.bfloat16)
    return (mixed_heads, new_state)

def layer_norm(values, gain):
    row_mean = lax.optimization_barrier(jnp.mean(values, -1, keepdims=True))
    square = lax.optimization_barrier(jnp.mean(values * values, -1, keepdims=True))
    return ((values - row_mean) * lax.rsqrt(square - row_mean * row_mean + NORM_EPS) * gain).astype(jnp.bfloat16)

def slot_numbers(route_ids, expert_count, capacity):
    onehot = (route_ids[..., None] == jnp.arange(expert_count, dtype=jnp.int32)).astype(jnp.int32)
    position = lax.optimization_barrier(jnp.sum(jnp.cumsum(onehot, -2) * onehot, -1)) - 1
    return route_ids * capacity + position

def take_rows(source_rows, row_index):
    return source_rows[row_index]

def one_expert(operands):
    rows_in, gate_mat, up_mat, down_mat = operands
    gate_part = jnp.dot(rows_in, gate_mat, preferred_element_type=jnp.float32)
    up_part = jnp.dot(rows_in, up_mat, preferred_element_type=jnp.float32)
    hidden = (jax.nn.silu(gate_part) * up_part).astype(jnp.bfloat16)
    return jnp.dot(hidden, down_mat, preferred_element_type=jnp.float32).astype(jnp.bfloat16)

def reference(tokens, retention_state, lengths, query_weight, key_weight, value_weight, gate_weight, out_weight, first_gain, routing, route_weight, expert_gate, expert_up, expert_down, shared_gate, shared_up, shared_down, side_gate, side_up, side_down, side_switch, second_gain):
    mixed_heads, new_state = retain(tokens, retention_state, lengths, query_weight, key_weight, value_weight, gate_weight, 0)
    mixing = jnp.dot(mixed_heads, out_weight, preferred_element_type=jnp.float32)
    normed = layer_norm(RESIDUAL_SCALE * tokens.astype(jnp.float32) + mixing, first_gain)
    shared_hidden = (jax.nn.silu(jnp.dot(normed, shared_gate, preferred_element_type=jnp.float32)) * jnp.dot(normed, shared_up, preferred_element_type=jnp.float32)).astype(jnp.bfloat16)
    shared_out = jnp.dot(shared_hidden, shared_down, preferred_element_type=jnp.float32)
    side_hidden = (jax.nn.silu(jnp.dot(normed, side_gate, preferred_element_type=jnp.float32)) * jnp.dot(normed, side_up, preferred_element_type=jnp.float32)).astype(jnp.bfloat16)
    side_out = jnp.dot(side_hidden, side_down, preferred_element_type=jnp.float32)
    switch = jax.nn.sigmoid(jnp.dot(normed, side_switch, preferred_element_type=jnp.float32))
    assigned = SEQ_DEV * TOPK
    groups = routing.reshape(N_EP, assigned)
    slot_ids = slot_numbers(groups, EXPERTS, CAP)
    owners = jnp.arange(assigned, dtype=jnp.int32) // TOPK
    table = jnp.full((N_EP, EXPERTS * CAP), SEQ_DEV, jnp.int32)
    table = table.at[jnp.arange(N_EP, dtype=jnp.int32)[:, None], slot_ids].set(jnp.broadcast_to(owners[None, :], (N_EP, assigned)))
    padded = jnp.concatenate([normed.reshape(N_EP, SEQ_DEV, D), jnp.zeros((N_EP, 1, D), jnp.bfloat16)], 1)
    slot_rows = jax.vmap(take_rows)(padded, table)
    per_expert = jnp.transpose(slot_rows.reshape(N_EP, EXPERTS, CAP, D), (1, 0, 2, 3)).reshape(EXPERTS, N_EP * CAP, D)
    outputs = lax.map(one_expert, (per_expert, expert_gate, expert_up, expert_down))
    back = jnp.transpose(outputs.reshape(EXPERTS, N_EP, CAP, D), (1, 0, 2, 3)).reshape(N_EP, EXPERTS * CAP, D)
    picked = jax.vmap(take_rows)(back, slot_ids).reshape(BATCH, TOPK, D)
    routed = lax.optimization_barrier(jnp.sum(picked.astype(jnp.float32) * route_weight[:, :, None], 1))
    pre_second = RESIDUAL_SCALE * normed.astype(jnp.float32) + routed + shared_out + switch[:, None] * side_out
    output = layer_norm(pre_second, second_gain)
    return (output, new_state)
```

```python
import jax
import jax.numpy as jnp
from jax import lax
from jax.sharding import Mesh
from jax.sharding import PartitionSpec as P

HEADS = 16
TP = ("tp_0", "tp_1")


RESIDUAL_SCALE = 2.0**0.25
NORM_EPS = 1e-05
GROUP_EPS = 1e-06
ROPE_BASE = 10000.0


def in_order(parts, dim):
    parts = jnp.moveaxis(parts, 0, dim)
    dims = parts.shape
    return parts.reshape(*dims[:dim], dims[dim] * dims[dim + 1], *dims[dim + 2 :])


def rotate(vector, positions):
    half_width = vector.shape[-1] // 2
    frequency = ROPE_BASE ** (-jnp.arange(half_width, dtype=jnp.float32) / half_width)
    angles = positions.astype(jnp.float32)[:, None, None] * frequency[None, None, :]
    cosine = jnp.cos(angles)
    sine_part = jnp.sin(angles)
    first_half = vector[..., :half_width]
    second_half = vector[..., half_width:]
    return jnp.concatenate(
        [
            first_half * cosine - second_half * sine_part,
            second_half * cosine + first_half * sine_part,
        ],
        -1,
    )


def retain(
    tokens,
    retention_state,
    lengths,
    query_weight,
    key_weight,
    value_weight,
    gate_weight,
    first_head,
):
    row_count = tokens.shape[0]
    head_count = retention_state.shape[1]
    head_width = retention_state.shape[2]

    def project(weight):
        rounded = jnp.dot(tokens, weight, preferred_element_type=jnp.float32).astype(jnp.bfloat16)
        return lax.optimization_barrier(rounded).astype(jnp.float32)

    queries = rotate(project(query_weight).reshape(row_count, head_count, head_width), lengths)
    key_rows = rotate(
        project(key_weight).reshape(row_count, head_count, head_width), lengths
    ) * head_width ** (-0.5)
    values = project(value_weight).reshape(row_count, head_count, head_width)
    gate_act = project(gate_weight)
    head_index = (first_head + jnp.arange(head_count)).astype(jnp.float32)
    decays = 1.0 - 2.0 ** (-5.0 - 7.0 * head_index / (HEADS - 1))
    own_term = jnp.sum(queries * key_rows, -1, keepdims=True) * values
    carried = decays[None, :, None] * jnp.einsum("bhd,bhde->bhe", queries, retention_state)
    result = own_term + carried
    new_state = (
        decays[None, :, None, None] * retention_state
        + key_rows[:, :, :, None] * values[:, :, None, :]
    )
    normed = result * lax.rsqrt(jnp.mean(result * result, -1, keepdims=True) + GROUP_EPS)
    mixed_heads = (
        normed.reshape(row_count, head_count * head_width) * jax.nn.silu(gate_act)
    ).astype(jnp.bfloat16)
    return (mixed_heads, new_state)


EP = ("z", "core")
PITCH = 24
RIDER = 8


def swap(parts, axis):
    return lax.all_to_all(parts, axis, 0, 0, tiled=True)


def to_all(shard, axis):
    length = lax.axis_size(axis)
    return swap(jnp.broadcast_to(shard[None], (length, *shard.shape)), axis)


def after(value, other):
    return lax.optimization_barrier((value, other))[0]


def normalize(rows, gain, axes):
    count = 1
    for a in axes:
        count *= rows.shape[a]
    mean = jnp.sum(rows, axes, keepdims=True) / count
    square = jnp.sum(rows * rows, axes, keepdims=True) / count
    return (rows - mean) * lax.rsqrt(square - mean * mean + NORM_EPS) * gain, mean, square


def f32_dot(a, b, dims):
    return lax.dot_general(a, b, (dims, ((), ())), preferred_element_type=jnp.float32)


def on_device(
    tokens,
    retention_state,
    lengths,
    query_weight,
    key_weight,
    value_weight,
    gate_weight,
    out_weight,
    first_gain,
    routing,
    route_weight,
    expert_gate,
    expert_up,
    expert_down,
    shared_gate,
    shared_up,
    shared_down,
    side_gate,
    side_up,
    side_down,
    side_switch,
    second_gain,
):
    bf16 = jnp.bfloat16
    seq_rows, model_width = tokens.shape
    head_count = retention_state.shape[1]
    col_count = out_weight.shape[1]
    ep_count = lax.axis_size(EP)
    tp_count = lax.axis_size(TP)
    class_count = lax.axis_size("tp_1")
    part_count = lax.axis_size("tp_0")
    local_experts = expert_gate.shape[0]
    hidden_cols = expert_gate.shape[2]
    top_count = routing.shape[1]
    capacity = (3 * seq_rows * top_count + local_experts * ep_count - 1) // (local_experts * ep_count)
    slots = ep_count * capacity
    tp_rank = lax.axis_index(TP)
    col_start = tp_rank * col_count

    mixed_heads, new_state = retain(
        tokens,
        retention_state,
        lengths,
        query_weight,
        key_weight,
        value_weight,
        gate_weight,
        tp_rank * head_count,
    )
    mixed_all = in_order(to_all(mixed_heads, TP), 1)

    same = routing.reshape(-1)[:, None] == routing.reshape(-1)[None, :]
    row_of = jnp.arange(seq_rows * top_count, dtype=jnp.int32) // top_count
    earlier = row_of[None, :] < row_of[:, None]
    position = jnp.sum((same & earlier).astype(jnp.int32), 1).reshape(seq_rows, top_count)
    slot_ids = (
        (routing // local_experts) * PITCH + (routing % local_experts) * capacity + position
    )
    wire_ids = jnp.arange(ep_count * PITCH, dtype=jnp.int32)
    table = jnp.zeros((ep_count * PITCH, seq_rows), jnp.bool_)
    for k in range(top_count):
        table = table | (wire_ids[:, None] == slot_ids[None, :, k])
    table = table.astype(bf16)
    slot_hot = (slot_ids.T.reshape(-1)[:, None] == wire_ids[None, :]).astype(bf16)

    lane = lax.axis_index("tp_1")
    gate_up = (jnp.swapaxes(expert_gate, 1, 2), jnp.swapaxes(expert_up, 1, 2))

    def piece_for(expert):
        return jnp.stack([lax.dynamic_index_in_dim(w, expert, 0, False) for w in gate_up])

    pieces = [piece_for(lane)]
    for d in range(1, class_count):
        steps = [(i, (i + d) % class_count) for i in range(class_count)]
        pieces.append(lax.ppermute(piece_for((lane + d) % class_count), "tp_1", steps))
    gate_t, up_t = (jnp.concatenate([p[i] for p in pieces], 0) for i in range(2))
    down = expert_down.reshape(local_experts, part_count, class_count, hidden_cols, col_count)
    down = jnp.stack(
        [
            jnp.concatenate([down[j, :, (j - d) % class_count] for d in range(class_count)], 1)
            for j in range(local_experts)
        ]
    )

    mixing = jnp.dot(mixed_all, out_weight, preferred_element_type=jnp.float32)
    own_cols = lax.dynamic_slice_in_dim(tokens, col_start, col_count, 1).astype(jnp.float32)
    pre_first = RESIDUAL_SCALE * own_cols + mixing
    pre_short = pre_first.astype(bf16)

    side_cols = side_gate.shape[1]
    side_rows = side_gate.shape[0]
    core_count = lax.axis_size("core")
    side_piece = jnp.concatenate([side_gate.T, side_up.T], 1)
    rider = jnp.broadcast_to(
        side_piece.reshape(1, core_count, RIDER, 2 * side_rows),
        (ep_count // core_count, core_count, RIDER, 2 * side_rows),
    ).reshape(ep_count, RIDER, 2 * side_rows)
    outgoing = jnp.dot(table, pre_short, preferred_element_type=jnp.float32).astype(bf16)
    arrived = swap(
        jnp.concatenate([outgoing.reshape(ep_count, PITCH, col_count), rider], 1), EP
    )
    side_own = arrived[:, PITCH:]
    side_other = lax.ppermute(side_own, "core", [(0, 1), (1, 0)])
    first_core = lax.axis_index("core") == 0
    side_all = jnp.concatenate(
        [
            jnp.where(first_core, side_own, side_other),
            jnp.where(first_core, side_other, side_own),
        ],
        1,
    ).reshape(ep_count, side_cols, 2, side_rows)
    side_all = jnp.transpose(side_all, (2, 1, 0, 3)).reshape(2, side_cols, model_width)

    order = jnp.arange(local_experts * slots, dtype=jnp.int32)
    source, expert, place = (order % slots) // capacity, order // slots, order % capacity
    spot = expert * capacity + place
    came_at = source * (PITCH + RIDER) + spot
    regroup = (
        came_at[:, None] == jnp.arange(ep_count * (PITCH + RIDER), dtype=jnp.int32)[None, :]
    ).astype(bf16)
    by_expert = jnp.dot(
        regroup, arrived.reshape(-1, col_count), preferred_element_type=jnp.float32
    ).astype(bf16)
    own_too = jnp.concatenate(
        [
            by_expert.reshape(local_experts, slots, col_count),
            jnp.broadcast_to(pre_short[None], (local_experts, seq_rows, col_count)),
        ],
        1,
    )
    to_send = jnp.broadcast_to(own_too[None], (part_count, *own_too.shape))
    rows_pre = swap(to_send.reshape(tp_count, slots + seq_rows, col_count), TP)
    gains = first_gain.reshape(tp_count, 1, col_count)
    parts, mean, square = normalize(rows_pre.astype(jnp.float32), gains, (0, 2))
    normed_rows = in_order(parts.astype(bf16), 1)
    slot_rows, normed_full = normed_rows[:slots], normed_rows[slots:]
    mean, square = mean[0, slots:], square[0, slots:]
    own_gain = lax.dynamic_slice_in_dim(first_gain, col_start, col_count, 0)
    normed_cols = (
        (pre_first - mean) * lax.rsqrt(square - mean * mean + NORM_EPS) * own_gain
    ).astype(bf16)

    across = ((1,), (1,))
    hidden = (
        jax.nn.silu(f32_dot(slot_rows, gate_t, across)) * f32_dot(slot_rows, up_t, across)
    ).astype(bf16)
    side_hidden = (
        jax.nn.silu(f32_dot(normed_full, side_all[0], across))
        * f32_dot(normed_full, side_all[1], across)
    ).astype(bf16)
    shared_hidden = (
        jax.nn.silu(jnp.dot(normed_full, shared_gate, preferred_element_type=jnp.float32))
        * jnp.dot(normed_full, shared_up, preferred_element_type=jnp.float32)
    ).astype(bf16)
    switch = jax.nn.sigmoid(jnp.dot(normed_full, side_switch, preferred_element_type=jnp.float32))

    shared_cols = shared_hidden.shape[1]
    units = hidden.shape[1]
    spare = units - shared_cols - side_cols
    local_hidden = jnp.concatenate(
        [shared_hidden, side_hidden, jnp.zeros((seq_rows, spare), bf16)], 1
    )
    hidden_all = to_all(jnp.concatenate([hidden, local_hidden], 0), TP)
    expert_hidden = hidden_all[:, :slots].reshape(part_count, class_count, slots, units)
    local_all = in_order(hidden_all[:, slots:], 1)
    result = jnp.einsum("qjrf,jqfd->jrd", expert_hidden, down, preferred_element_type=jnp.float32)
    goes_at = source * PITCH + spot
    sent_back = jnp.dot(
        (wire_ids[:, None] == goes_at[None, :]).astype(bf16),
        result.astype(bf16).reshape(local_experts * slots, col_count),
        preferred_element_type=jnp.float32,
    ).astype(bf16)
    returned = swap(sent_back.reshape(ep_count, PITCH, col_count), EP)

    shared_part = jnp.pad(
        shared_down.reshape(tp_count, shared_cols, col_count),
        ((0, 0), (0, units - shared_cols), (0, 0)),
    ).reshape(tp_count * units, col_count)
    side_part = jnp.pad(
        side_down.reshape(tp_count, side_cols, col_count),
        ((0, 0), (shared_cols, spare), (0, 0)),
    ).reshape(tp_count * units, col_count)
    shared_out = jnp.dot(local_all, shared_part, preferred_element_type=jnp.float32)
    side_out = jnp.dot(local_all, side_part, preferred_element_type=jnp.float32)
    local_sum = (
        RESIDUAL_SCALE * normed_cols.astype(jnp.float32) + shared_out + switch[:, None] * side_out
    )

    picked = jnp.dot(
        slot_hot, returned.reshape(-1, col_count), preferred_element_type=jnp.float32
    ).reshape(top_count, seq_rows, col_count)
    routed = jnp.sum(picked * route_weight.T[:, :, None], 0)
    pre_second = local_sum + routed
    sums = jnp.stack([jnp.sum(pre_second, -1), jnp.sum(pre_second * pre_second, -1)])
    totals = jnp.sum(to_all(sums, TP), 0)
    mean_second = totals[0][:, None] / model_width
    square_second = totals[1][:, None] / model_width
    output = (
        (pre_second - mean_second)
        * lax.rsqrt(square_second - mean_second * mean_second + NORM_EPS)
        * second_gain
    ).astype(bf16)
    return (output, new_state)


def solution(mesh):
    chips = mesh.devices.reshape(mesh.shape["ep"] // 2, 2, 4, 4)
    finer = Mesh(chips, (*EP, *TP))
    return jax.shard_map(
        on_device,
        mesh=finer,
        in_specs=(
            P(EP, None),
            P(EP, TP, None, None),
            P(EP),
            P(None, TP),
            P(None, TP),
            P(None, TP),
            P(None, TP),
            P(None, TP),
            P(),
            P(EP, None),
            P(EP, None),
            P(EP, None, TP),
            P(EP, None, TP),
            P(EP, None, TP),
            P(None, TP),
            P(None, TP),
            P(None, TP),
            P(EP, TP),
            P(EP, TP),
            P(None, TP),
            P(),
            P(TP),
        ),
        out_specs=(P(EP, TP), P(EP, TP, None, None)),
        check_vma=False,
    )
```

```python
import jax
import jax.numpy as jnp
from jax import lax
from jax.experimental import pallas as pl
from jax.experimental.pallas import tpu as pltpu
from jax.sharding import Mesh
from jax.sharding import PartitionSpec as P

HEADS = 16
TP = ("tp_0", "tp_1")


RESIDUAL_SCALE = 2.0**0.25
NORM_EPS = 1e-05
GROUP_EPS = 1e-06
ROPE_BASE = 10000.0
ACROSS = ((1,), (1,))


def in_order(parts, dim):
    parts = jnp.moveaxis(parts, 0, dim)
    dims = parts.shape
    return parts.reshape(*dims[:dim], dims[dim] * dims[dim + 1], *dims[dim + 2 :])


def rotate(vector, positions):
    half_width = vector.shape[-1] // 2
    frequency = ROPE_BASE ** (-jnp.arange(half_width, dtype=jnp.float32) / half_width)
    angles = positions.astype(jnp.float32)[:, None, None] * frequency[None, None, :]
    cosine = jnp.cos(angles)
    sine_part = jnp.sin(angles)
    first_half = vector[..., :half_width]
    second_half = vector[..., half_width:]
    return jnp.concatenate(
        [
            first_half * cosine - second_half * sine_part,
            second_half * cosine + first_half * sine_part,
        ],
        -1,
    )


def project_kernel(tokens, *refs):
    weights, out, total = refs[:-2], refs[-2], refs[-1]
    step = pl.program_id(0)

    @pl.when(step == 0)
    def _():
        total[...] = jnp.zeros_like(total)

    stacked = jnp.concatenate([w[...] for w in weights], 0)
    total[...] += f32_dot(tokens[...], stacked, ACROSS)

    @pl.when(step == pl.num_programs(0) - 1)
    def _():
        out[...] = total[...].astype(out.dtype)


def project_all(tokens, weights):
    rows, width = tokens.shape
    cols = weights[0].shape[1]
    steps = 4
    span = width // steps
    return pl.pallas_call(
        project_kernel,
        grid=(steps,),
        in_specs=[pl.BlockSpec((rows, span), lambda i: (0, i))]
        + [pl.BlockSpec((cols, span), lambda i: (0, i)) for _ in weights],
        out_specs=pl.BlockSpec((rows, cols * len(weights)), lambda i: (0, 0)),
        out_shape=jax.ShapeDtypeStruct((rows, cols * len(weights)), jnp.bfloat16),
        scratch_shapes=[pltpu.VMEM((rows, cols * len(weights)), jnp.float32)],
        name="project",
    )(tokens, *[w.T for w in weights])


def retain(
    tokens,
    retention_state,
    lengths,
    query_weight,
    key_weight,
    value_weight,
    gate_weight,
    first_head,
):
    row_count = tokens.shape[0]
    head_count = retention_state.shape[1]
    head_width = retention_state.shape[2]

    projected = project_all(tokens, (query_weight, key_weight, value_weight, gate_weight))
    queries, keys, values, gate_act = jnp.split(projected.astype(jnp.float32), 4, 1)
    by_head = (row_count, head_count, head_width)
    queries = rotate(queries.reshape(by_head), lengths)
    key_rows = rotate(keys.reshape(by_head), lengths) * head_width ** (-0.5)
    values = values.reshape(by_head)
    head_index = (first_head + jnp.arange(head_count)).astype(jnp.float32)
    decays = 1.0 - 2.0 ** (-5.0 - 7.0 * head_index / (HEADS - 1))
    own_term = jnp.sum(queries * key_rows, -1, keepdims=True) * values
    carried = decays[None, :, None] * jnp.einsum("bhd,bhde->bhe", queries, retention_state)
    result = own_term + carried
    new_state = (
        decays[None, :, None, None] * retention_state
        + key_rows[:, :, :, None] * values[:, :, None, :]
    )
    normed = result * lax.rsqrt(jnp.mean(result * result, -1, keepdims=True) + GROUP_EPS)
    mixed_heads = (
        normed.reshape(row_count, head_count * head_width) * jax.nn.silu(gate_act)
    ).astype(jnp.bfloat16)
    return (mixed_heads, new_state)


EP = ("z", "core")
PITCH = 24
RIDER = 8


def swap(parts, axis):
    return lax.all_to_all(parts, axis, 0, 0, tiled=True)


def to_all(shard, axis):
    length = lax.axis_size(axis)
    return swap(jnp.broadcast_to(shard[None], (length, *shard.shape)), axis)


def f32_dot(a, b, dims):
    return lax.dot_general(a, b, (dims, ((), ())), preferred_element_type=jnp.float32)


def hidden_kernel(rows_pre, gains, pre_first, own_gain, local_weights, *refs):
    pieces, (hidden, normed_cols, switch, normed) = refs[:-4], refs[-4:]
    parts, row_count, cols = rows_pre.shape
    own_rows = pre_first.shape[0]
    slots = row_count - own_rows
    width = parts * cols
    total = jnp.zeros((row_count, cols), jnp.float32)
    total_square = jnp.zeros((row_count, cols), jnp.float32)
    for t in range(parts):
        block = rows_pre[t].astype(jnp.float32)
        total = total + block
        total_square = total_square + block * block
    mean = jnp.sum(total, -1, keepdims=True) / width
    square = jnp.sum(total_square, -1, keepdims=True) / width
    scale = lax.rsqrt(square - mean * mean + NORM_EPS)
    for t in range(parts):
        block = (rows_pre[t].astype(jnp.float32) - mean) * scale * gains[t : t + 1]
        normed[:, t * cols : (t + 1) * cols] = block.astype(normed.dtype)
    normed_cols[...] = ((pre_first[...] - mean[slots:]) * scale[slots:] * own_gain[...]).astype(
        normed_cols.dtype
    )
    gate_up = jnp.concatenate([p[i] for i in range(2) for p in pieces], 0)
    units = gate_up.shape[0] // 2
    both = f32_dot(normed[:slots], gate_up, ACROSS)
    hidden[:slots] = (jax.nn.silu(both[:, :units]) * both[:, units:]).astype(hidden.dtype)
    local = f32_dot(normed[slots:], local_weights[...], ACROSS)
    cut = (local.shape[1] - RIDER) // 2
    mine = jax.nn.silu(local[:, :cut]) * local[:, cut : 2 * cut]
    hidden[slots:] = jnp.zeros((own_rows, units), hidden.dtype)
    hidden[slots:, :cut] = mine.astype(hidden.dtype)
    switch[...] = jax.nn.sigmoid(local[:, 2 * cut : 2 * cut + 1])


def hidden_units(rows_pre, gains, pre_first, own_gain, local_weights, pieces):
    parts, row_count, cols = rows_pre.shape
    units = sum(p.shape[1] for p in pieces)
    own_rows = pre_first.shape[0]
    whole = pl.BlockSpec(memory_space=pltpu.VMEM)
    return pl.pallas_call(
        hidden_kernel,
        in_specs=[whole] * (5 + len(pieces)),
        out_specs=[whole] * 3,
        out_shape=[
            jax.ShapeDtypeStruct((row_count, units), jnp.bfloat16),
            jax.ShapeDtypeStruct((own_rows, cols), jnp.bfloat16),
            jax.ShapeDtypeStruct((own_rows, 1), jnp.float32),
        ],
        scratch_shapes=[pltpu.VMEM((row_count, parts * cols), jnp.bfloat16)],
        name="hidden_units",
    )(rows_pre, gains, pre_first, own_gain, local_weights, *pieces)


def on_device(
    tokens,
    retention_state,
    lengths,
    query_weight,
    key_weight,
    value_weight,
    gate_weight,
    out_weight,
    first_gain,
    routing,
    route_weight,
    expert_gate,
    expert_up,
    expert_down,
    shared_gate,
    shared_up,
    shared_down,
    side_gate,
    side_up,
    side_down,
    side_switch,
    second_gain,
):
    bf16 = jnp.bfloat16
    seq_rows, model_width = tokens.shape
    head_count = retention_state.shape[1]
    col_count = out_weight.shape[1]
    ep_count = lax.axis_size(EP)
    tp_count = lax.axis_size(TP)
    class_count = lax.axis_size("tp_1")
    part_count = lax.axis_size("tp_0")
    local_experts = expert_gate.shape[0]
    hidden_cols = expert_gate.shape[2]
    top_count = routing.shape[1]
    capacity = (3 * seq_rows * top_count + local_experts * ep_count - 1) // (local_experts * ep_count)
    slots = ep_count * capacity
    tp_rank = lax.axis_index(TP)
    col_start = tp_rank * col_count

    mixed_heads, new_state = retain(
        tokens,
        retention_state,
        lengths,
        query_weight,
        key_weight,
        value_weight,
        gate_weight,
        tp_rank * head_count,
    )
    head_width = mixed_heads.shape[1]
    half = seq_rows // 2
    folded = jnp.concatenate([mixed_heads[:half], mixed_heads[half:]], 1)
    folded_all = to_all(folded, TP)
    left = jnp.arange(2 * head_width, dtype=jnp.int32)[None, None, :] < head_width
    none = jnp.zeros_like(folded_all)
    mixed_all = in_order(
        jnp.concatenate(
            [jnp.where(left, folded_all, none), jnp.where(left, none, folded_all)], 1
        ),
        1,
    )
    head_weight = out_weight.reshape(tp_count, 1, head_width, col_count)
    head_weight = jnp.broadcast_to(head_weight, (tp_count, 2, head_width, col_count))
    head_weight = head_weight.reshape(tp_count * 2 * head_width, col_count)

    same = routing.reshape(-1)[:, None] == routing.reshape(-1)[None, :]
    row_of = jnp.arange(seq_rows * top_count, dtype=jnp.int32) // top_count
    earlier = row_of[None, :] < row_of[:, None]
    position = jnp.sum((same & earlier).astype(jnp.int32), 1).reshape(seq_rows, top_count)
    slot_ids = (
        (routing // local_experts) * PITCH + (routing % local_experts) * capacity + position
    )
    wire_ids = jnp.arange(ep_count * PITCH, dtype=jnp.int32)
    table = jnp.zeros((ep_count * PITCH, seq_rows), jnp.bool_)
    for k in range(top_count):
        table = table | (wire_ids[:, None] == slot_ids[None, :, k])
    table = table.astype(bf16)
    slot_hot = (slot_ids.T.reshape(-1)[:, None] == wire_ids[None, :]).astype(bf16)

    lane = lax.axis_index("tp_1")
    gate_up = (jnp.swapaxes(expert_gate, 1, 2), jnp.swapaxes(expert_up, 1, 2))

    def piece_for(expert):
        return jnp.stack([lax.dynamic_index_in_dim(w, expert, 0, False) for w in gate_up])

    pieces = [piece_for(lane)]
    for d in range(1, class_count):
        steps = [(i, (i + d) % class_count) for i in range(class_count)]
        pieces.append(lax.ppermute(piece_for((lane + d) % class_count), "tp_1", steps))
    down = expert_down.reshape(local_experts, part_count, class_count, hidden_cols, col_count)
    down = jnp.stack(
        [
            jnp.concatenate([down[j, :, (j - d) % class_count] for d in range(class_count)], 1)
            for j in range(local_experts)
        ]
    )

    mixing = jnp.dot(mixed_all, head_weight, preferred_element_type=jnp.float32)
    own_cols = lax.dynamic_slice_in_dim(tokens, col_start, col_count, 1).astype(jnp.float32)
    pre_first = RESIDUAL_SCALE * own_cols + mixing
    pre_short = pre_first.astype(bf16)

    side_cols = side_gate.shape[1]
    side_rows = side_gate.shape[0]
    core_count = lax.axis_size("core")
    side_piece = jnp.concatenate([side_gate.T, side_up.T], 1)
    rider = jnp.broadcast_to(
        side_piece.reshape(1, core_count, RIDER, 2 * side_rows),
        (ep_count // core_count, core_count, RIDER, 2 * side_rows),
    ).reshape(ep_count, RIDER, 2 * side_rows)
    outgoing = jnp.dot(table, pre_short, preferred_element_type=jnp.float32).astype(bf16)
    arrived = swap(jnp.concatenate([outgoing.reshape(ep_count, PITCH, col_count), rider], 1), EP)
    side_own = arrived[:, PITCH:]
    side_other = lax.ppermute(side_own, "core", [(0, 1), (1, 0)])
    first_core = lax.axis_index("core") == 0
    side_all = jnp.concatenate(
        [
            jnp.where(first_core, side_own, side_other),
            jnp.where(first_core, side_other, side_own),
        ],
        1,
    ).reshape(ep_count, side_cols, 2, side_rows)
    side_all = jnp.transpose(side_all, (2, 1, 0, 3)).reshape(2, side_cols, model_width)

    order = jnp.arange(local_experts * slots, dtype=jnp.int32)
    source, expert, place = (order % slots) // capacity, order // slots, order % capacity
    spot = expert * capacity + place
    came_at = source * (PITCH + RIDER) + spot
    regroup = (
        came_at[:, None] == jnp.arange(ep_count * (PITCH + RIDER), dtype=jnp.int32)[None, :]
    ).astype(bf16)
    by_expert = jnp.dot(
        regroup, arrived.reshape(-1, col_count), preferred_element_type=jnp.float32
    ).astype(bf16)
    own_too = jnp.concatenate(
        [
            by_expert.reshape(local_experts, slots, col_count),
            jnp.broadcast_to(pre_short[None], (local_experts, seq_rows, col_count)),
        ],
        1,
    )
    to_send = jnp.broadcast_to(own_too[None], (part_count, *own_too.shape))
    rows_pre = swap(to_send.reshape(tp_count, slots + seq_rows, col_count), TP)
    own_gain = lax.dynamic_slice_in_dim(first_gain, col_start, col_count, 0)
    units = class_count * hidden_cols
    shared_cols = shared_gate.shape[1]
    spare = units - shared_cols - side_cols
    local_weights = jnp.concatenate(
        [
            shared_gate.T,
            side_all[0],
            shared_up.T,
            side_all[1],
            jnp.broadcast_to(side_switch[None], (RIDER, model_width)),
        ],
        0,
    )
    hidden, normed_cols, switch = hidden_units(
        rows_pre, first_gain.reshape(tp_count, col_count), pre_first, own_gain[None], local_weights, pieces
    )

    hidden_all = to_all(hidden, TP)
    expert_hidden = hidden_all[:, :slots].reshape(part_count, class_count, slots, units)
    local_all = in_order(hidden_all[:, slots:], 1)
    result = jnp.einsum("qjrf,jqfd->jrd", expert_hidden, down, preferred_element_type=jnp.float32)
    goes_at = source * PITCH + spot
    sent_back = jnp.dot(
        (wire_ids[:, None] == goes_at[None, :]).astype(bf16),
        result.astype(bf16).reshape(local_experts * slots, col_count),
        preferred_element_type=jnp.float32,
    ).astype(bf16)
    returned = swap(sent_back.reshape(ep_count, PITCH, col_count), EP)

    shared_part = jnp.pad(
        shared_down.reshape(tp_count, shared_cols, col_count),
        ((0, 0), (0, units - shared_cols), (0, 0)),
    ).reshape(tp_count * units, col_count)
    side_part = jnp.pad(
        side_down.reshape(tp_count, side_cols, col_count),
        ((0, 0), (shared_cols, spare), (0, 0)),
    ).reshape(tp_count * units, col_count)
    shared_out = jnp.dot(local_all, shared_part, preferred_element_type=jnp.float32)
    side_out = jnp.dot(local_all, side_part, preferred_element_type=jnp.float32)
    local_sum = (
        RESIDUAL_SCALE * normed_cols.astype(jnp.float32) + shared_out + switch * side_out
    )

    picked = jnp.dot(
        slot_hot, returned.reshape(-1, col_count), preferred_element_type=jnp.float32
    ).reshape(top_count, seq_rows, col_count)
    routed = jnp.sum(picked * route_weight.T[:, :, None], 0)
    pre_second = local_sum + routed
    sums = jnp.stack([jnp.sum(pre_second, -1), jnp.sum(pre_second * pre_second, -1)])
    totals = jnp.sum(to_all(sums, TP), 0)
    mean_second = totals[0][:, None] / model_width
    square_second = totals[1][:, None] / model_width
    output = (
        (pre_second - mean_second)
        * lax.rsqrt(square_second - mean_second * mean_second + NORM_EPS)
        * second_gain
    ).astype(bf16)
    return (output, new_state)


def solution(mesh):
    chips = mesh.devices.reshape(mesh.shape["ep"] // 2, 2, 4, 4)
    finer = Mesh(chips, (*EP, *TP))

    return jax.shard_map(
        on_device,
        mesh=finer,
        in_specs=(
            P(EP, None),
            P(EP, TP, None, None),
            P(EP),
            P(None, TP),
            P(None, TP),
            P(None, TP),
            P(None, TP),
            P(None, TP),
            P(),
            P(EP, None),
            P(EP, None),
            P(EP, None, TP),
            P(EP, None, TP),
            P(EP, None, TP),
            P(None, TP),
            P(None, TP),
            P(None, TP),
            P(EP, TP),
            P(EP, TP),
            P(None, TP),
            P(),
            P(TP),
        ),
        out_specs=(P(EP, TP), P(EP, TP, None, None)),
        check_vma=False,
    )
```

```python
import jax
import jax.numpy as jnp
from jax import lax
from jax.experimental import pallas as pl
from jax.experimental.pallas import tpu as pltpu
from jax.sharding import Mesh
from jax.sharding import PartitionSpec as P

HEADS = 16
TP = ("tp_0", "tp_1")


RESIDUAL_SCALE = 2.0**0.25
NORM_EPS = 1e-05
GROUP_EPS = 1e-06
ROPE_BASE = 10000.0
ACROSS = ((1,), (1,))


def in_order(parts, dim):
    parts = jnp.moveaxis(parts, 0, dim)
    dims = parts.shape
    return parts.reshape(*dims[:dim], dims[dim] * dims[dim + 1], *dims[dim + 2 :])


def rotate(vector, positions):
    half_width = vector.shape[-1] // 2
    frequency = ROPE_BASE ** (-jnp.arange(half_width, dtype=jnp.float32) / half_width)
    angles = positions[:, None, None] * frequency[None, None, :]
    cosine = jnp.cos(angles)
    sine_part = jnp.sin(angles)
    first_half = vector[..., :half_width]
    second_half = vector[..., half_width:]
    return jnp.concatenate(
        [
            first_half * cosine - second_half * sine_part,
            second_half * cosine + first_half * sine_part,
        ],
        -1,
    )


def near(*arrays):
    return [pltpu.with_memory_space_constraint(a, pltpu.VMEM) for a in arrays]


def project_kernel(tokens, lengths, *refs):
    count = (len(refs) - 4) // 2
    weights, (out, positions) = refs[:count], refs[count : count + 2]
    rows, held, arrived = refs[count + 2], refs[count + 3 : -1], refs[-1]
    fetch = [
        pltpu.make_async_copy(source, target, arrived.at[i])
        for i, (source, target) in enumerate(zip((tokens, *weights), (rows, *held)))
    ]
    for f in fetch:
        f.start()
    positions[...] = lengths[...].astype(jnp.float32)
    fetch[0].wait()
    for i, w in enumerate(held):
        fetch[i + 1].wait()
        cols = w.shape[0]
        part = f32_dot(rows[...], w[...], ACROSS).astype(jnp.bfloat16)
        out[:, i * cols : (i + 1) * cols] = part.astype(jnp.float32)


def project_all(tokens, lengths, weights):
    rows, width = tokens.shape
    cols = weights[0].shape[1]
    count = len(weights)
    anywhere = pl.BlockSpec(memory_space=pl.ANY)
    whole = pl.BlockSpec(memory_space=pltpu.VMEM)
    return pl.pallas_call(
        project_kernel,
        in_specs=[anywhere, whole] + [anywhere] * count,
        out_specs=[whole, whole],
        out_shape=[
            pltpu.VMEM((rows, cols * count), jnp.float32),
            pltpu.VMEM(lengths.shape, jnp.float32),
        ],
        scratch_shapes=[pltpu.VMEM((rows, width), tokens.dtype)]
        + [pltpu.VMEM((cols, width), weights[0].dtype)] * count
        + [pltpu.SemaphoreType.DMA((count + 1,))],
        name="project",
    )(tokens, lengths, *[w.T for w in weights])


def dispatch_kernel(folded_all, out_weight, own_cols, table, rider, outgoing, exact, short, lhs, rhs):
    parts, half, lanes = folded_all.shape
    width = lanes // 2
    lane = lax.broadcasted_iota(jnp.int32, (half, lanes), 1)
    for t in range(parts):
        block = folded_all[t].astype(jnp.float32)
        at = slice(t * lanes, (t + 1) * lanes)
        lhs[0, :, at] = jnp.where(lane < width, block, 0.0).astype(lhs.dtype)
        lhs[1, :, at] = jnp.where(lane < width, 0.0, block).astype(lhs.dtype)
        for i in range(2):
            rhs[t * lanes + i * width : t * lanes + (i + 1) * width] = out_weight[
                t * width : (t + 1) * width
            ]
    flat = ((1,), (0,))
    mixing = jnp.concatenate([f32_dot(lhs[i], rhs[...], flat) for i in range(2)], 0)
    pre_first = RESIDUAL_SCALE * own_cols[...].astype(jnp.float32) + mixing
    exact[...] = pre_first
    pre_short = pre_first.astype(short.dtype)
    short[...] = pre_short
    peers, _, cols = outgoing.shape
    rows = f32_dot(table[...], pre_short, flat).reshape(peers, PITCH, cols)
    riders = rider[...].astype(jnp.float32)
    riders = jnp.broadcast_to(riders[None], (peers // riders.shape[0], *riders.shape))
    riders = riders.reshape(peers, RIDER, cols)
    outgoing[...] = jnp.concatenate([rows, riders], 1).astype(outgoing.dtype)


def dispatch_rows(folded_all, out_weight, own_cols, table, rider, peers):
    parts, half, lanes = folded_all.shape
    rows, cols = own_cols.shape
    bf16 = jnp.bfloat16
    whole = pl.BlockSpec(memory_space=pltpu.VMEM)
    return pl.pallas_call(
        dispatch_kernel,
        in_specs=[whole] * 5,
        out_specs=[whole] * 3,
        out_shape=[
            jax.ShapeDtypeStruct((peers, PITCH + RIDER, cols), bf16),
            pltpu.VMEM((rows, cols), jnp.float32),
            pltpu.VMEM((rows, cols), bf16),
        ],
        scratch_shapes=[
            pltpu.VMEM((2, half, parts * lanes), bf16),
            pltpu.VMEM((parts * lanes, cols), bf16),
        ],
        name="dispatch_rows",
    )(*near(folded_all, out_weight, own_cols, table, rider))


def return_kernel(hidden_all, down, goes, sent_back):
    parts, experts = down.shape[1], down.shape[0]
    slots = goes.shape[1] // experts
    flat = ((1,), (0,))
    results = []
    for j in range(experts):
        rows = jnp.concatenate([hidden_all[q * experts + j, :slots] for q in range(parts)], 1)
        mats = jnp.concatenate([down[j, q] for q in range(parts)], 0)
        results.append(f32_dot(rows, mats, flat).astype(sent_back.dtype))
    back = f32_dot(goes[...], jnp.concatenate(results, 0), flat)
    sent_back[...] = back.reshape(sent_back.shape).astype(sent_back.dtype)


def return_rows(hidden_all, down, goes, peers):
    cols = down.shape[-1]
    whole = pl.BlockSpec(memory_space=pltpu.VMEM)
    return pl.pallas_call(
        return_kernel,
        in_specs=[whole] * 3,
        out_specs=whole,
        out_shape=jax.ShapeDtypeStruct((peers, goes.shape[0] // peers, cols), jnp.bfloat16),
        name="return_rows",
    )(*near(hidden_all, down, goes))


def retain(
    tokens,
    retention_state,
    lengths,
    query_weight,
    key_weight,
    value_weight,
    gate_weight,
    first_head,
):
    row_count = tokens.shape[0]
    head_count = retention_state.shape[1]
    head_width = retention_state.shape[2]

    projected, positions = project_all(
        tokens, lengths, (query_weight, key_weight, value_weight, gate_weight)
    )
    queries, keys, values, gate_act = jnp.split(projected, 4, 1)
    by_head = (row_count, head_count, head_width)
    queries = rotate(queries.reshape(by_head), positions)
    key_rows = rotate(keys.reshape(by_head), positions) * head_width ** (-0.5)
    values = values.reshape(by_head)
    head_index = (first_head + jnp.arange(head_count)).astype(jnp.float32)
    decays = 1.0 - 2.0 ** (-5.0 - 7.0 * head_index / (HEADS - 1))
    own_term = jnp.sum(queries * key_rows, -1, keepdims=True) * values
    carried = decays[None, :, None] * jnp.einsum("bhd,bhde->bhe", queries, retention_state)
    result = own_term + carried
    new_state = (
        decays[None, :, None, None] * retention_state
        + key_rows[:, :, :, None] * values[:, :, None, :]
    )
    normed = result * lax.rsqrt(jnp.mean(result * result, -1, keepdims=True) + GROUP_EPS)
    mixed_heads = (
        normed.reshape(row_count, head_count * head_width) * jax.nn.silu(gate_act)
    ).astype(jnp.bfloat16)
    return (mixed_heads, new_state)


EP = ("z", "core")
PITCH = 24
RIDER = 8


def swap(parts, axis):
    return lax.all_to_all(parts, axis, 0, 0, tiled=True)


def to_all(shard, axis):
    length = lax.axis_size(axis)
    return swap(jnp.broadcast_to(shard[None], (length, *shard.shape)), axis)


def f32_dot(a, b, dims):
    return lax.dot_general(a, b, (dims, ((), ())), preferred_element_type=jnp.float32)


def hidden_kernel(rows_pre, gains, pre_first, own_gain, local_weights, *refs):
    pieces, (message, normed_cols, switch, normed, hidden, sent) = refs[:-6], refs[-6:]
    parts, row_count, cols = rows_pre.shape
    own_rows = pre_first.shape[0]
    slots = row_count - own_rows
    width = parts * cols
    total = jnp.zeros((row_count, cols), jnp.float32)
    total_square = jnp.zeros((row_count, cols), jnp.float32)
    for t in range(parts):
        block = rows_pre[t].astype(jnp.float32)
        total = total + block
        total_square = total_square + block * block
    mean = jnp.sum(total, -1, keepdims=True) / width
    square = jnp.sum(total_square, -1, keepdims=True) / width
    scale = lax.rsqrt(square - mean * mean + NORM_EPS)
    for t in range(parts):
        block = (rows_pre[t].astype(jnp.float32) - mean) * scale * gains[t : t + 1]
        normed[:, t * cols : (t + 1) * cols] = block.astype(normed.dtype)
    normed_cols[...] = ((pre_first[...] - mean[slots:]) * scale[slots:] * own_gain[...]).astype(
        normed_cols.dtype
    )
    gate_up = jnp.concatenate([p[i] for i in range(2) for p in pieces], 0)
    units = gate_up.shape[0] // 2
    both = f32_dot(normed[:slots], gate_up, ACROSS)
    hidden[:slots] = (jax.nn.silu(both[:, :units]) * both[:, units:]).astype(hidden.dtype)
    local = f32_dot(normed[slots:], local_weights[...], ACROSS)
    cut = (local.shape[1] - RIDER) // 2
    mine = jax.nn.silu(local[:, :cut]) * local[:, cut : 2 * cut]
    mine = jnp.concatenate([mine, jnp.zeros((own_rows, units // 2 - cut), jnp.float32)], 1)
    half = own_rows // 2
    hidden[slots:] = jnp.concatenate([mine[:half], mine[half:]], 1).astype(hidden.dtype)
    copies = [
        pltpu.make_async_copy(hidden, message.at[t], sent.at[t]) for t in range(message.shape[0])
    ]
    for c in copies:
        c.start()
    switch[...] = jax.nn.sigmoid(local[:, 2 * cut : 2 * cut + 1])
    for c in copies:
        c.wait()


def hidden_units(rows_pre, gains, pre_first, own_gain, local_weights, pieces):
    parts, row_count, cols = rows_pre.shape
    units = sum(p.shape[1] for p in pieces)
    own_rows = pre_first.shape[0]
    whole = pl.BlockSpec(memory_space=pltpu.VMEM)
    return pl.pallas_call(
        hidden_kernel,
        in_specs=[whole] * (5 + len(pieces)),
        out_specs=[pl.BlockSpec(memory_space=pl.ANY), whole, whole],
        out_shape=[
            jax.ShapeDtypeStruct((parts, row_count - own_rows // 2, units), jnp.bfloat16),
            pltpu.VMEM((own_rows, cols), jnp.bfloat16),
            pltpu.VMEM((own_rows, 1), jnp.float32),
        ],
        scratch_shapes=[
            pltpu.VMEM((row_count, parts * cols), jnp.bfloat16),
            pltpu.VMEM((row_count - own_rows // 2, units), jnp.bfloat16),
            pltpu.SemaphoreType.DMA((parts,)),
        ],
        name="hidden_units",
    )(*near(rows_pre, gains, pre_first, own_gain, local_weights, *pieces))


def on_device(
    tokens,
    retention_state,
    lengths,
    query_weight,
    key_weight,
    value_weight,
    gate_weight,
    out_weight,
    first_gain,
    routing,
    route_weight,
    expert_gate,
    expert_up,
    expert_down,
    shared_gate,
    shared_up,
    shared_down,
    side_gate,
    side_up,
    side_down,
    side_switch,
    second_gain,
):
    bf16 = jnp.bfloat16
    seq_rows, model_width = tokens.shape
    head_count = retention_state.shape[1]
    col_count = out_weight.shape[1]
    ep_count = lax.axis_size(EP)
    tp_count = lax.axis_size(TP)
    class_count = lax.axis_size("tp_1")
    part_count = lax.axis_size("tp_0")
    local_experts = expert_gate.shape[0]
    hidden_cols = expert_gate.shape[2]
    top_count = routing.shape[1]
    capacity = (3 * seq_rows * top_count + local_experts * ep_count - 1) // (local_experts * ep_count)
    slots = ep_count * capacity
    tp_rank = lax.axis_index(TP)
    col_start = tp_rank * col_count

    mixed_heads, new_state = retain(
        tokens,
        retention_state,
        lengths,
        query_weight,
        key_weight,
        value_weight,
        gate_weight,
        tp_rank * head_count,
    )
    half = seq_rows // 2
    folded = jnp.concatenate([mixed_heads[:half], mixed_heads[half:]], 1)
    folded_all = to_all(folded, TP)

    same = routing.reshape(-1)[:, None] == routing.reshape(-1)[None, :]
    row_of = jnp.arange(seq_rows * top_count, dtype=jnp.int32) // top_count
    earlier = row_of[None, :] < row_of[:, None]
    position = jnp.sum((same & earlier).astype(jnp.int32), 1).reshape(seq_rows, top_count)
    slot_ids = (
        (routing // local_experts) * PITCH + (routing % local_experts) * capacity + position
    )
    wire_ids = jnp.arange(ep_count * PITCH, dtype=jnp.int32)
    table = jnp.zeros((ep_count * PITCH, seq_rows), jnp.bool_)
    for k in range(top_count):
        table = table | (wire_ids[:, None] == slot_ids[None, :, k])
    table = table.astype(bf16)
    slot_hot = (slot_ids.T.reshape(-1)[:, None] == wire_ids[None, :]).astype(bf16)

    lane = lax.axis_index("tp_1")
    gate_up = (jnp.swapaxes(expert_gate, 1, 2), jnp.swapaxes(expert_up, 1, 2))

    def piece_for(expert):
        return jnp.stack([lax.dynamic_index_in_dim(w, expert, 0, False) for w in gate_up])

    pieces = [piece_for(lane)]
    for d in range(1, class_count):
        steps = [(i, (i + d) % class_count) for i in range(class_count)]
        pieces.append(lax.ppermute(piece_for((lane + d) % class_count), "tp_1", steps))
    down = expert_down.reshape(local_experts, part_count, class_count, hidden_cols, col_count)
    down = jnp.stack(
        [
            jnp.concatenate([down[j, :, (j - d) % class_count] for d in range(class_count)], 1)
            for j in range(local_experts)
        ]
    )

    own_cols = lax.dynamic_slice_in_dim(tokens, col_start, col_count, 1)

    side_cols = side_gate.shape[1]
    side_rows = side_gate.shape[0]
    core_count = lax.axis_size("core")
    side_piece = jnp.concatenate([side_gate.T, side_up.T], 1)
    outgoing, pre_first, pre_short = dispatch_rows(
        folded_all,
        out_weight,
        own_cols,
        table,
        side_piece.reshape(core_count, RIDER, 2 * side_rows),
        ep_count,
    )
    arrived = swap(outgoing, EP)
    side_own = arrived[:, PITCH:]
    side_other = lax.ppermute(side_own, "core", [(0, 1), (1, 0)])
    first_core = lax.axis_index("core") == 0
    side_all = jnp.concatenate(
        [
            jnp.where(first_core, side_own, side_other),
            jnp.where(first_core, side_other, side_own),
        ],
        1,
    ).reshape(ep_count, side_cols, 2, side_rows)
    side_all = jnp.transpose(side_all, (2, 1, 0, 3)).reshape(2, side_cols, model_width)

    order = jnp.arange(local_experts * slots, dtype=jnp.int32)
    source, expert, place = (order % slots) // capacity, order // slots, order % capacity
    spot = expert * capacity + place
    came_at = source * (PITCH + RIDER) + spot
    regroup = (
        came_at[:, None] == jnp.arange(ep_count * (PITCH + RIDER), dtype=jnp.int32)[None, :]
    ).astype(bf16)
    by_expert = jnp.dot(
        regroup, arrived.reshape(-1, col_count), preferred_element_type=jnp.float32
    ).astype(bf16)
    own_too = jnp.concatenate(
        [
            by_expert.reshape(local_experts, slots, col_count),
            jnp.broadcast_to(pre_short[None], (local_experts, seq_rows, col_count)),
        ],
        1,
    )
    to_send = jnp.broadcast_to(own_too[None], (part_count, *own_too.shape))
    rows_pre = swap(to_send.reshape(tp_count, slots + seq_rows, col_count), TP)
    own_gain = lax.dynamic_slice_in_dim(first_gain, col_start, col_count, 0)
    units = class_count * hidden_cols
    shared_cols = shared_gate.shape[1]
    local_weights = jnp.concatenate(
        [
            shared_gate.T,
            side_all[0],
            shared_up.T,
            side_all[1],
            jnp.broadcast_to(side_switch[None], (RIDER, model_width)),
        ],
        0,
    )
    hidden, normed_cols, switch = hidden_units(
        rows_pre, first_gain.reshape(tp_count, col_count), pre_first, own_gain[None], local_weights, pieces
    )

    hidden_all = swap(hidden, TP)
    goes_at = source * PITCH + spot
    goes = (wire_ids[:, None] == goes_at[None, :]).astype(bf16)
    down = down.reshape(local_experts, part_count, units, col_count)
    returned = swap(return_rows(hidden_all, down, goes, ep_count), EP)

    local_all = hidden_all[:, slots:]
    left = jnp.arange(units, dtype=jnp.int32)[None, None, :] < units // 2
    none = jnp.zeros_like(local_all)
    local_all = in_order(
        jnp.concatenate([jnp.where(left, local_all, none), jnp.where(left, none, local_all)], 1), 1
    )

    def spread(weight, first):
        count = weight.shape[0] // tp_count
        weight = jnp.pad(
            weight.reshape(tp_count, 1, count, col_count),
            ((0, 0), (0, 0), (first, units // 2 - first - count), (0, 0)),
        )
        weight = jnp.broadcast_to(weight, (tp_count, 2, units // 2, col_count))
        return weight.reshape(tp_count * units, col_count)

    shared_out = jnp.dot(
        local_all, spread(shared_down, 0), preferred_element_type=jnp.float32
    )
    side_out = jnp.dot(
        local_all, spread(side_down, shared_cols), preferred_element_type=jnp.float32
    )
    local_sum = (
        RESIDUAL_SCALE * normed_cols.astype(jnp.float32) + shared_out + switch * side_out
    )

    picked = jnp.dot(
        slot_hot, returned.reshape(-1, col_count), preferred_element_type=jnp.float32
    ).reshape(top_count, seq_rows, col_count)
    routed = jnp.sum(picked * route_weight.T[:, :, None], 0)
    pre_second = local_sum + routed
    sums = jnp.stack([jnp.sum(pre_second, -1), jnp.sum(pre_second * pre_second, -1)])
    totals = jnp.sum(to_all(sums, TP), 0)
    mean_second = totals[0][:, None] / model_width
    square_second = totals[1][:, None] / model_width
    output = (
        (pre_second - mean_second)
        * lax.rsqrt(square_second - mean_second * mean_second + NORM_EPS)
        * second_gain
    ).astype(bf16)
    return (output, new_state)


def solution(mesh):
    chips = mesh.devices.reshape(mesh.shape["ep"] // 2, 2, 4, 4)
    finer = Mesh(chips, (*EP, *TP))

    return jax.shard_map(
        on_device,
        mesh=finer,
        in_specs=(
            P(EP, None),
            P(EP, TP, None, None),
            P(EP),
            P(None, TP),
            P(None, TP),
            P(None, TP),
            P(None, TP),
            P(None, TP),
            P(),
            P(EP, None),
            P(EP, None),
            P(EP, None, TP),
            P(EP, None, TP),
            P(EP, None, TP),
            P(None, TP),
            P(None, TP),
            P(None, TP),
            P(EP, TP),
            P(EP, TP),
            P(None, TP),
            P(),
            P(TP),
        ),
        out_specs=(P(EP, TP), P(EP, TP, None, None)),
        check_vma=False,
    )
```

```python
import jax
import jax.numpy as jnp
from jax import lax
from jax.experimental import pallas as pl
from jax.experimental.pallas import tpu as pltpu
from jax.sharding import Mesh
from jax.sharding import PartitionSpec as P

HEADS = 16
TP = ("tp_0", "tp_1")


RESIDUAL_SCALE = 2.0**0.25
NORM_EPS = 1e-05
GROUP_EPS = 1e-06
ROPE_BASE = 10000.0
ACROSS = ((1,), (1,))
EP = ("z", "core")
PITCH = 24
RIDER = 8
FLAT = ((1,), (0,))
GROUP = 8
GRANT = 12 * 1024 * 1024


def in_order(parts, dim):
    parts = jnp.moveaxis(parts, 0, dim)
    dims = parts.shape
    return parts.reshape(*dims[:dim], dims[dim] * dims[dim + 1], *dims[dim + 2 :])


def rotate(vector, positions):
    half_width = vector.shape[-1] // 2
    frequency = ROPE_BASE ** (-jnp.arange(half_width, dtype=jnp.float32) / half_width)
    angles = positions[:, None, None] * frequency[None, None, :]
    cosine = jnp.cos(angles)
    sine_part = jnp.sin(angles)
    first_half = vector[..., :half_width]
    second_half = vector[..., half_width:]
    return jnp.concatenate(
        [
            first_half * cosine - second_half * sine_part,
            second_half * cosine + first_half * sine_part,
        ],
        -1,
    )


def near(*arrays):
    return [pltpu.with_memory_space_constraint(a, pltpu.VMEM) for a in arrays]


def far(*arrays):
    return [pltpu.with_memory_space_constraint(a, pltpu.HBM) for a in arrays]


def project_kernel(tokens, lengths, *refs):
    count = (len(refs) - 6) // 2
    weights, outs = refs[:count], refs[count:-6]
    positions, own_cols, rows, held, counts, arrived = refs[-6:]
    cols, width = weights[0].shape
    long = pltpu.make_async_copy(lengths, counts, arrived.at[2, 0])
    span = width // 2
    fetch = []
    for h in range(2):
        at = pl.ds(h * span, span)
        fetch.append(
            [pltpu.make_async_copy(tokens.at[:, at], rows.at[:, at], arrived.at[h, 0])]
            + [
                pltpu.make_async_copy(
                    w.at[:, at], held.at[pl.ds(i * cols, cols), at], arrived.at[h, i + 1]
                )
                for i, w in enumerate(weights)
            ]
        )
        for f in fetch[h]:
            f.start()
    long.start()
    total = None
    for h, group in enumerate(fetch):
        for f in group:
            f.wait()
        at = slice(h * span, (h + 1) * span)
        part = f32_dot(rows[:, at], held[:, at], ACROSS)
        total = part if total is None else total + part
    column = lax.axis_index("tp_0") * lax.axis_size("tp_1") + lax.axis_index("tp_1")
    size = own_cols.shape[1]
    own_cols[...] = rows[:, pl.ds(pl.multiple_of(column * size, size), size)]
    long.wait()
    positions[...] = counts[...].astype(jnp.float32)
    rounded = total.astype(jnp.bfloat16).astype(jnp.float32)
    for i, out in enumerate(outs):
        out[...] = rounded[:, i * cols : (i + 1) * cols]


def project_all(tokens, lengths, weights, parts):
    rows, width = tokens.shape
    cols = weights[0].shape[1]
    count = len(weights)
    anywhere = pl.BlockSpec(memory_space=pl.ANY)
    whole = pl.BlockSpec(memory_space=pltpu.VMEM)
    return pl.pallas_call(
        project_kernel,
        in_specs=[anywhere] * (count + 2),
        out_specs=[whole] * (count + 2),
        out_shape=[pltpu.VMEM((rows, cols), jnp.float32)] * count
        + [
            pltpu.VMEM(lengths.shape, jnp.float32),
            pltpu.VMEM((rows, width // parts), tokens.dtype),
        ],
        scratch_shapes=[
            pltpu.VMEM((rows, width), tokens.dtype),
            pltpu.VMEM((cols * count, width), weights[0].dtype),
            pltpu.VMEM(lengths.shape, lengths.dtype),
            pltpu.SemaphoreType.DMA((3, count + 1)),
        ],
        name="project",
        compiler_params=pltpu.CompilerParams(vmem_limit_bytes=GRANT),
    )(*far(tokens, lengths, *[w.T for w in weights]))


def dispatch_kernel(
    folded_all, out_weight, table, rider, own_cols, outgoing, exact, short, lhs, rhs
):
    parts, half, lanes = folded_all.shape
    cols = out_weight.shape[1]
    width = lanes // 2
    lane = lax.broadcasted_iota(jnp.int32, (half, lanes), 1)
    for t in range(parts):
        block = folded_all[t].astype(jnp.float32)
        at = slice(t * lanes, (t + 1) * lanes)
        lhs[0, :, at] = jnp.where(lane < width, block, 0.0).astype(lhs.dtype)
        lhs[1, :, at] = jnp.where(lane < width, 0.0, block).astype(lhs.dtype)
        for i in range(2):
            rhs[t * lanes + i * width : t * lanes + (i + 1) * width] = out_weight[
                t * width : (t + 1) * width
            ]
    mixing = jnp.concatenate([f32_dot(lhs[i], rhs[...], FLAT) for i in range(2)], 0)
    pre_first = RESIDUAL_SCALE * own_cols[...].astype(jnp.float32) + mixing
    exact[...] = pre_first
    pre_short = pre_first.astype(short.dtype)
    short[...] = pre_short
    peers = outgoing.shape[0]
    rows = f32_dot(table[...], pre_short, FLAT).reshape(peers, PITCH, cols)
    riders = rider[...].astype(jnp.float32)
    riders = jnp.broadcast_to(riders[None], (peers // riders.shape[0], *riders.shape))
    riders = riders.reshape(peers, RIDER, cols)
    outgoing[...] = jnp.concatenate([rows, riders], 1).astype(outgoing.dtype)


def dispatch_rows(folded_all, out_weight, table, rider, own_cols, peers):
    parts, half, lanes = folded_all.shape
    rows, cols = own_cols.shape
    bf16 = jnp.bfloat16
    whole = pl.BlockSpec(memory_space=pltpu.VMEM)
    return pl.pallas_call(
        dispatch_kernel,
        in_specs=[whole] * 5,
        out_specs=[whole] * 3,
        out_shape=[
            jax.ShapeDtypeStruct((peers, PITCH + RIDER, cols), bf16),
            pltpu.VMEM((rows, cols), jnp.float32),
            pltpu.VMEM((rows, cols), bf16),
        ],
        scratch_shapes=[
            pltpu.VMEM((2, half, parts * lanes), bf16),
            pltpu.VMEM((parts * lanes, cols), bf16),
        ],
        name="dispatch_rows",
        compiler_params=pltpu.CompilerParams(vmem_limit_bytes=GRANT),
    )(*near(folded_all, out_weight, table, rider, own_cols))


def pieces_kernel(ready, gate_t, up_t, *refs):
    del ready
    pieces, moved = refs[:-1], refs[-1]
    experts = gate_t.shape[0]
    lane = lax.axis_index("tp_1")
    moves = [
        pltpu.make_async_copy(w.at[(lane + d) % experts], piece.at[i], moved.at[d, i])
        for d, piece in enumerate(pieces)
        for i, w in enumerate((gate_t, up_t))
    ]
    for m in moves:
        m.start()
    for m in moves:
        m.wait()


def expert_pieces(ready, gate_t, up_t):
    experts, units, width = gate_t.shape
    anywhere = pl.BlockSpec(memory_space=pl.ANY)
    whole = pl.BlockSpec(memory_space=pltpu.VMEM)
    return pl.pallas_call(
        pieces_kernel,
        in_specs=[whole] + [anywhere] * 2,
        out_specs=[whole] * experts,
        out_shape=[pltpu.VMEM((2, units, width), gate_t.dtype)] * experts,
        scratch_shapes=[pltpu.SemaphoreType.DMA((experts, 2))],
        name="expert_pieces",
        compiler_params=pltpu.CompilerParams(vmem_limit_bytes=GRANT),
    )(*near(ready), *far(gate_t, up_t))


def mixed_kernel(result, gate_act, message, folded, sent):
    value = result[...]
    scale = lax.rsqrt(jnp.mean(value * value, -1, keepdims=True) + GROUP_EPS)
    mixed = value * scale * jax.nn.silu(gate_act[...])
    half = mixed.shape[0] // 2
    folded[...] = jnp.concatenate([mixed[:half], mixed[half:]], 1).astype(folded.dtype)
    copies = [
        pltpu.make_async_copy(folded, message.at[t], sent.at[t]) for t in range(message.shape[0])
    ]
    for c in copies:
        c.start()
    for c in copies:
        c.wait()


def mixed_message(result, gate_act, peers):
    rows, width = result.shape
    whole = pl.BlockSpec(memory_space=pltpu.VMEM)
    return pl.pallas_call(
        mixed_kernel,
        in_specs=[whole] * 2,
        out_specs=pl.BlockSpec(memory_space=pl.ANY),
        out_shape=jax.ShapeDtypeStruct((peers, rows // 2, 2 * width), jnp.bfloat16),
        scratch_shapes=[
            pltpu.VMEM((rows // 2, 2 * width), jnp.bfloat16),
            pltpu.SemaphoreType.DMA((peers,)),
        ],
        name="mixed_message",
        compiler_params=pltpu.CompilerParams(vmem_limit_bytes=GRANT),
    )(*near(result, gate_act))


def slot_kernel(arrived, own, regroup, message, rows, sent):
    experts, row_count, cols = rows.shape
    peers, pitch, _ = arrived.shape
    slots = row_count - own.shape[0]
    groups = peers // GROUP
    count = slots // groups
    for j in range(experts):
        rows[j, slots:] = own[...]
    for g in range(groups):
        block = arrived[g * GROUP : (g + 1) * GROUP].reshape(GROUP * pitch, cols)
        moved = f32_dot(regroup[...], block, FLAT).astype(rows.dtype)
        for j in range(experts):
            rows[j, g * count : (g + 1) * count] = moved[j * count : (j + 1) * count]
    copies = [
        pltpu.make_async_copy(rows, message.at[q], sent.at[q]) for q in range(message.shape[0])
    ]
    for c in copies:
        c.start()
    for c in copies:
        c.wait()


def slot_message(arrived, own, regroup, experts, slots, copies):
    cols = own.shape[1]
    whole = pl.BlockSpec(memory_space=pltpu.VMEM)
    rows = slots + own.shape[0]
    return pl.pallas_call(
        slot_kernel,
        in_specs=[whole] * 3,
        out_specs=pl.BlockSpec(memory_space=pl.ANY),
        out_shape=jax.ShapeDtypeStruct((copies, experts, rows, cols), jnp.bfloat16),
        scratch_shapes=[
            pltpu.VMEM((experts, rows, cols), jnp.bfloat16),
            pltpu.SemaphoreType.DMA((copies,)),
        ],
        name="slot_message",
        compiler_params=pltpu.CompilerParams(vmem_limit_bytes=GRANT),
    )(*near(arrived, own, regroup))


def return_kernel(hidden_all, down, goes, sent_back):
    parts, experts = down.shape[1], down.shape[0]
    peers, pitch, cols = sent_back.shape
    groups = peers // GROUP
    count = goes.shape[1] // experts
    slots = count * groups
    results = []
    for j in range(experts):
        rows = jnp.concatenate([hidden_all[q * experts + j, :slots] for q in range(parts)], 1)
        mats = jnp.concatenate([down[j, q] for q in range(parts)], 0)
        results.append(f32_dot(rows, mats, FLAT))
    for g in range(groups):
        block = jnp.concatenate([r[g * count : (g + 1) * count] for r in results], 0)
        back = f32_dot(goes[...], block.astype(sent_back.dtype), FLAT)
        sent_back[g * GROUP : (g + 1) * GROUP] = back.reshape(GROUP, pitch, cols).astype(
            sent_back.dtype
        )


def return_rows(hidden_all, down, goes, peers):
    cols = down.shape[-1]
    whole = pl.BlockSpec(memory_space=pltpu.VMEM)
    return pl.pallas_call(
        return_kernel,
        in_specs=[whole] * 3,
        out_specs=whole,
        out_shape=jax.ShapeDtypeStruct((peers, PITCH, cols), jnp.bfloat16),
        name="return_rows",
        compiler_params=pltpu.CompilerParams(vmem_limit_bytes=GRANT),
    )(*near(hidden_all, down, goes))


def retain(
    tokens,
    retention_state,
    lengths,
    query_weight,
    key_weight,
    value_weight,
    gate_weight,
    first_head,
):
    row_count = tokens.shape[0]
    head_count = retention_state.shape[1]
    head_width = retention_state.shape[2]

    queries, keys, values, gate_act, positions, own_cols = project_all(
        tokens, lengths, (query_weight, key_weight, value_weight, gate_weight), lax.axis_size(TP)
    )
    by_head = (row_count, head_count, head_width)
    queries = rotate(queries.reshape(by_head), positions)
    key_rows = rotate(keys.reshape(by_head), positions) * head_width ** (-0.5)
    values = values.reshape(by_head)
    head_index = (first_head + jnp.arange(head_count)).astype(jnp.float32)
    decays = 1.0 - 2.0 ** (-5.0 - 7.0 * head_index / (HEADS - 1))
    own_term = jnp.sum(queries * key_rows, -1, keepdims=True) * values
    carried = decays[None, :, None] * jnp.einsum("bhd,bhde->bhe", queries, retention_state)
    result = own_term + carried
    new_state = (
        decays[None, :, None, None] * retention_state
        + key_rows[:, :, :, None] * values[:, :, None, :]
    )
    result = result.reshape(row_count, head_count * head_width)
    return (mixed_message(result, gate_act, lax.axis_size(TP)), new_state, own_cols)


def swap(parts, axis):
    return lax.all_to_all(parts, axis, 0, 0, tiled=True)


def to_all(shard, axis):
    length = lax.axis_size(axis)
    return swap(jnp.broadcast_to(shard[None], (length, *shard.shape)), axis)


def f32_dot(a, b, dims):
    return lax.dot_general(a, b, (dims, ((), ())), preferred_element_type=jnp.float32)


def hidden_kernel(rows_pre, gains, pre_first, own_gain, local_weights, *refs):
    pieces, (message, normed_cols, switch, normed, hidden, gate_up, sent) = refs[:-7], refs[-7:]
    parts, row_count, cols = rows_pre.shape
    own_rows = pre_first.shape[0]
    slots = row_count - own_rows
    width = parts * cols
    total = jnp.zeros((row_count, cols), jnp.float32)
    total_square = jnp.zeros((row_count, cols), jnp.float32)
    for t in range(parts):
        block = rows_pre[t].astype(jnp.float32)
        total = total + block
        total_square = total_square + block * block
    mean = jnp.sum(total, -1, keepdims=True) / width
    square = jnp.sum(total_square, -1, keepdims=True) / width
    scale = lax.rsqrt(square - mean * mean + NORM_EPS)
    for t in range(parts):
        block = (rows_pre[t].astype(jnp.float32) - mean) * scale * gains[t : t + 1]
        normed[:, t * cols : (t + 1) * cols] = block.astype(normed.dtype)
    normed_cols[...] = ((pre_first[...] - mean[slots:]) * scale[slots:] * own_gain[...]).astype(
        normed_cols.dtype
    )
    units = gate_up.shape[0] // 2
    lane = lax.axis_index("tp_1")
    for d, piece in enumerate(pieces):
        span = piece.shape[1]
        start = (lane + len(pieces) - d) % len(pieces) * span
        for i in range(2):
            gate_up[pl.ds(pl.multiple_of(i * units + start, span), span)] = piece[i]
    both = f32_dot(normed[:slots], gate_up[...], ACROSS)
    hidden[:slots] = (jax.nn.silu(both[:, :units]) * both[:, units:]).astype(hidden.dtype)
    local = f32_dot(normed[slots:], local_weights[...], ACROSS)
    cut = (local.shape[1] - RIDER) // 2
    mine = jax.nn.silu(local[:, :cut]) * local[:, cut : 2 * cut]
    mine = jnp.concatenate([mine, jnp.zeros((own_rows, units // 2 - cut), jnp.float32)], 1)
    half = own_rows // 2
    hidden[slots:] = jnp.concatenate([mine[:half], mine[half:]], 1).astype(hidden.dtype)
    copies = [
        pltpu.make_async_copy(hidden, message.at[t], sent.at[t]) for t in range(message.shape[0])
    ]
    for c in copies:
        c.start()
    switch[...] = jax.nn.sigmoid(local[:, 2 * cut : 2 * cut + 1])
    for c in copies:
        c.wait()


def hidden_units(rows_pre, gains, pre_first, own_gain, local_weights, pieces):
    parts, row_count, cols = rows_pre.shape
    units = sum(p.shape[1] for p in pieces)
    own_rows = pre_first.shape[0]
    whole = pl.BlockSpec(memory_space=pltpu.VMEM)
    return pl.pallas_call(
        hidden_kernel,
        in_specs=[whole] * (5 + len(pieces)),
        out_specs=[pl.BlockSpec(memory_space=pl.ANY), whole, whole],
        out_shape=[
            jax.ShapeDtypeStruct((parts, row_count - own_rows // 2, units), jnp.bfloat16),
            pltpu.VMEM((own_rows, cols), jnp.bfloat16),
            pltpu.VMEM((own_rows, 1), jnp.float32),
        ],
        scratch_shapes=[
            pltpu.VMEM((row_count, parts * cols), jnp.bfloat16),
            pltpu.VMEM((row_count - own_rows // 2, units), jnp.bfloat16),
            pltpu.VMEM((2 * units, parts * cols), jnp.bfloat16),
            pltpu.SemaphoreType.DMA((parts,)),
        ],
        name="hidden_units",
        compiler_params=pltpu.CompilerParams(vmem_limit_bytes=GRANT),
    )(*near(rows_pre, gains, pre_first, own_gain, local_weights, *pieces))


def on_device(
    tokens,
    retention_state,
    lengths,
    query_weight,
    key_weight,
    value_weight,
    gate_weight,
    out_weight,
    first_gain,
    routing,
    route_weight,
    expert_gate,
    expert_up,
    expert_down,
    shared_gate,
    shared_up,
    shared_down,
    side_gate,
    side_up,
    side_down,
    side_switch,
    second_gain,
):
    bf16 = jnp.bfloat16
    seq_rows, model_width = tokens.shape
    head_count = retention_state.shape[1]
    col_count = out_weight.shape[1]
    ep_count = lax.axis_size(EP)
    tp_count = lax.axis_size(TP)
    class_count = lax.axis_size("tp_1")
    part_count = lax.axis_size("tp_0")
    local_experts = expert_gate.shape[0]
    hidden_cols = expert_gate.shape[2]
    top_count = routing.shape[1]
    capacity = (3 * seq_rows * top_count + local_experts * ep_count - 1) // (local_experts * ep_count)
    slots = ep_count * capacity
    tp_rank = lax.axis_index(TP)
    col_start = tp_rank * col_count

    folded, new_state, own_cols = retain(
        tokens,
        retention_state,
        lengths,
        query_weight,
        key_weight,
        value_weight,
        gate_weight,
        tp_rank * head_count,
    )
    folded_all = swap(folded, TP)

    same = routing.reshape(-1)[:, None] == routing.reshape(-1)[None, :]
    row_of = jnp.arange(seq_rows * top_count, dtype=jnp.int32) // top_count
    earlier = row_of[None, :] < row_of[:, None]
    position = jnp.sum((same & earlier).astype(jnp.int32), 1).reshape(seq_rows, top_count)
    slot_ids = (
        (routing // local_experts) * PITCH + (routing % local_experts) * capacity + position
    )
    wire_ids = jnp.arange(ep_count * PITCH, dtype=jnp.int32)
    table = jnp.zeros((ep_count * PITCH, seq_rows), jnp.bool_)
    for k in range(top_count):
        table = table | (wire_ids[:, None] == slot_ids[None, :, k])
    table = table.astype(bf16)
    slot_hot = (slot_ids.T.reshape(-1)[:, None] == wire_ids[None, :]).astype(bf16)

    side_cols = side_gate.shape[1]
    side_rows = side_gate.shape[0]
    core_count = lax.axis_size("core")
    side_piece = jnp.concatenate([side_gate.T, side_up.T], 1)
    outgoing, pre_first, pre_short = dispatch_rows(
        folded_all,
        out_weight,
        table,
        side_piece.reshape(core_count, RIDER, 2 * side_rows),
        own_cols,
        ep_count,
    )
    pieces = list(
        expert_pieces(
            pre_short, jnp.swapaxes(expert_gate, 1, 2), jnp.swapaxes(expert_up, 1, 2)
        )
    )
    for d in range(1, class_count):
        steps = [(i, (i + d) % class_count) for i in range(class_count)]
        pieces[d] = lax.ppermute(pieces[d], "tp_1", steps)
    arrived = swap(outgoing, EP)
    side_own = arrived[:, PITCH:]
    side_other = lax.ppermute(side_own, "core", [(0, 1), (1, 0)])
    first_core = lax.axis_index("core") == 0
    side_all = jnp.concatenate(
        [
            jnp.where(first_core, side_own, side_other),
            jnp.where(first_core, side_other, side_own),
        ],
        1,
    ).reshape(ep_count, side_cols, 2, side_rows)
    side_all = jnp.transpose(side_all, (2, 1, 0, 3)).reshape(2, side_cols, model_width)

    order = jnp.arange(local_experts * GROUP * capacity, dtype=jnp.int32)
    expert, source = order // (GROUP * capacity), order // capacity % GROUP
    spot = expert * capacity + order % capacity
    came_at = source * (PITCH + RIDER) + spot
    regroup = (
        came_at[:, None] == jnp.arange(GROUP * (PITCH + RIDER), dtype=jnp.int32)[None, :]
    ).astype(bf16)
    to_send = slot_message(arrived, pre_short, regroup, local_experts, slots, part_count)
    rows_pre = swap(to_send.reshape(tp_count, slots + seq_rows, col_count), TP)
    own_gain = lax.dynamic_slice_in_dim(first_gain, col_start, col_count, 0)
    units = class_count * hidden_cols
    shared_cols = shared_gate.shape[1]
    local_weights = jnp.concatenate(
        [
            shared_gate.T,
            side_all[0],
            shared_up.T,
            side_all[1],
            jnp.broadcast_to(side_switch[None], (RIDER, model_width)),
        ],
        0,
    )
    hidden, normed_cols, switch = hidden_units(
        rows_pre, first_gain.reshape(tp_count, col_count), pre_first, own_gain[None], local_weights, pieces
    )

    hidden_all = swap(hidden, TP)
    goes_at = source * PITCH + spot
    goes = (wire_ids[: GROUP * PITCH, None] == goes_at[None, :]).astype(bf16)
    down = expert_down.reshape(local_experts, part_count, units, col_count)
    returned = swap(return_rows(hidden_all, down, goes, ep_count), EP)

    local_all = hidden_all[:, slots:]
    left = jnp.arange(units, dtype=jnp.int32)[None, None, :] < units // 2
    none = jnp.zeros_like(local_all)
    local_all = in_order(
        jnp.concatenate([jnp.where(left, local_all, none), jnp.where(left, none, local_all)], 1), 1
    )

    def spread(weight, first):
        count = weight.shape[0] // tp_count
        weight = jnp.pad(
            weight.reshape(tp_count, 1, count, col_count),
            ((0, 0), (0, 0), (first, units // 2 - first - count), (0, 0)),
        )
        weight = jnp.broadcast_to(weight, (tp_count, 2, units // 2, col_count))
        return weight.reshape(tp_count * units, col_count)

    shared_out = jnp.dot(
        local_all, spread(shared_down, 0), preferred_element_type=jnp.float32
    )
    side_out = jnp.dot(
        local_all, spread(side_down, shared_cols), preferred_element_type=jnp.float32
    )
    local_sum = (
        RESIDUAL_SCALE * normed_cols.astype(jnp.float32) + shared_out + switch * side_out
    )

    picked = jnp.dot(
        slot_hot, returned.reshape(-1, col_count), preferred_element_type=jnp.float32
    ).reshape(top_count, seq_rows, col_count)
    routed = jnp.sum(picked * route_weight.T[:, :, None], 0)
    pre_second = local_sum + routed
    sums = jnp.stack([jnp.sum(pre_second, -1), jnp.sum(pre_second * pre_second, -1)])
    sums, new_state = lax.optimization_barrier((sums, new_state))
    totals = jnp.sum(to_all(sums, TP), 0)
    mean_second = totals[0][:, None] / model_width
    square_second = totals[1][:, None] / model_width
    output = (
        (pre_second - mean_second)
        * lax.rsqrt(square_second - mean_second * mean_second + NORM_EPS)
        * second_gain
    ).astype(bf16)
    return (output, new_state)


def solution(mesh):
    chips = mesh.devices.reshape(mesh.shape["ep"] // 2, 2, 4, 4)
    finer = Mesh(chips, (*EP, *TP))

    return jax.shard_map(
        on_device,
        mesh=finer,
        in_specs=(
            P(EP, None),
            P(EP, TP, None, None),
            P(EP),
            P(None, TP),
            P(None, TP),
            P(None, TP),
            P(None, TP),
            P(None, TP),
            P(),
            P(EP, None),
            P(EP, None),
            P(EP, None, TP),
            P(EP, None, TP),
            P(EP, None, TP),
            P(None, TP),
            P(None, TP),
            P(None, TP),
            P(EP, TP),
            P(EP, TP),
            P(None, TP),
            P(),
            P(TP),
        ),
        out_specs=(P(EP, TP), P(EP, TP, None, None)),
        check_vma=False,
    )
```

```python
import jax
import jax.numpy as jnp
from jax import lax
from jax.experimental import pallas as pl
from jax.experimental.pallas import tpu as pltpu
from jax.sharding import Mesh
from jax.sharding import PartitionSpec as P

HEADS = 16
TP = ("tp_0", "tp_1")


RESIDUAL_SCALE = 2.0**0.25
NORM_EPS = 1e-05
GROUP_EPS = 1e-06
ROPE_BASE = 10000.0
ACROSS = ((1,), (1,))
EP = ("z", "core")
RIDER = 8
TILE = 4
FLAT = ((1,), (0,))
GROUP = 8
GRANT = 12 * 1024 * 1024


def in_order(parts, dim):
    parts = jnp.moveaxis(parts, 0, dim)
    dims = parts.shape
    return parts.reshape(*dims[:dim], dims[dim] * dims[dim + 1], *dims[dim + 2 :])


def rotate(vector, positions):
    half_width = vector.shape[-1] // 2
    frequency = ROPE_BASE ** (-jnp.arange(half_width, dtype=jnp.float32) / half_width)
    angles = positions[:, None, None] * frequency[None, None, :]
    cosine = jnp.cos(angles)
    sine_part = jnp.sin(angles)
    first_half = vector[..., :half_width]
    second_half = vector[..., half_width:]
    return jnp.concatenate(
        [
            first_half * cosine - second_half * sine_part,
            second_half * cosine + first_half * sine_part,
        ],
        -1,
    )


def near(*arrays):
    return [pltpu.with_memory_space_constraint(a, pltpu.VMEM) for a in arrays]


def far(*arrays):
    return [pltpu.with_memory_space_constraint(a, pltpu.HBM) for a in arrays]


def project_kernel(tokens, lengths, *refs):
    count = (len(refs) - 6) // 2
    weights, outs = refs[:count], refs[count:-6]
    positions, own_cols, rows, held, counts, arrived = refs[-6:]
    cols, width = weights[0].shape
    long = pltpu.make_async_copy(lengths, counts, arrived.at[2, 0])
    span = width // 2
    fetch = []
    for h in range(2):
        at = pl.ds(h * span, span)
        fetch.append(
            [pltpu.make_async_copy(tokens.at[:, at], rows.at[:, at], arrived.at[h, 0])]
            + [
                pltpu.make_async_copy(
                    w.at[:, at], held.at[pl.ds(i * cols, cols), at], arrived.at[h, i + 1]
                )
                for i, w in enumerate(weights)
            ]
        )
        for f in fetch[h]:
            f.start()
    long.start()
    total = None
    for h, group in enumerate(fetch):
        for f in group:
            f.wait()
        at = slice(h * span, (h + 1) * span)
        part = f32_dot(rows[:, at], held[:, at], ACROSS)
        total = part if total is None else total + part
    column = lax.axis_index("tp_0") * lax.axis_size("tp_1") + lax.axis_index("tp_1")
    size = own_cols.shape[1]
    own_cols[...] = rows[:, pl.ds(pl.multiple_of(column * size, size), size)]
    long.wait()
    positions[...] = counts[...].astype(jnp.float32)
    rounded = total.astype(jnp.bfloat16).astype(jnp.float32)
    for i, out in enumerate(outs):
        out[...] = rounded[:, i * cols : (i + 1) * cols]


def project_all(tokens, lengths, weights, parts):
    rows, width = tokens.shape
    cols = weights[0].shape[1]
    count = len(weights)
    anywhere = pl.BlockSpec(memory_space=pl.ANY)
    whole = pl.BlockSpec(memory_space=pltpu.VMEM)
    return pl.pallas_call(
        project_kernel,
        in_specs=[anywhere] * (count + 2),
        out_specs=[whole] * (count + 2),
        out_shape=[pltpu.VMEM((rows, cols), jnp.float32)] * count
        + [
            pltpu.VMEM(lengths.shape, jnp.float32),
            pltpu.VMEM((rows, width // parts), tokens.dtype),
        ],
        scratch_shapes=[
            pltpu.VMEM((rows, width), tokens.dtype),
            pltpu.VMEM((cols * count, width), weights[0].dtype),
            pltpu.VMEM(lengths.shape, lengths.dtype),
            pltpu.SemaphoreType.DMA((3, count + 1)),
        ],
        name="project",
        compiler_params=pltpu.CompilerParams(vmem_limit_bytes=GRANT),
    )(*far(tokens, lengths, *[w.T for w in weights]))


def dispatch_kernel(
    folded_all, out_weight, table, side_piece, own_cols, outgoing, exact, short, lhs, rhs
):
    parts, half, lanes = folded_all.shape
    width = lanes // 2
    lane = lax.broadcasted_iota(jnp.int32, (half, lanes), 1)
    for t in range(parts):
        block = folded_all[t].astype(jnp.float32)
        at = slice(t * lanes, (t + 1) * lanes)
        lhs[0, :, at] = jnp.where(lane < width, block, 0.0).astype(lhs.dtype)
        lhs[1, :, at] = jnp.where(lane < width, 0.0, block).astype(lhs.dtype)
        for i in range(2):
            rhs[t * lanes + i * width : t * lanes + (i + 1) * width] = out_weight[
                t * width : (t + 1) * width
            ]
    mixing = jnp.concatenate([f32_dot(lhs[i], rhs[...], FLAT) for i in range(2)], 0)
    pre_first = RESIDUAL_SCALE * own_cols[...].astype(jnp.float32) + mixing
    exact[...] = pre_first
    pre_short = pre_first.astype(short.dtype)
    short[...] = pre_short
    chosen = jnp.concatenate([pre_first, side_piece[...].astype(jnp.float32)], 0)
    outgoing[...] = f32_dot(table[...], chosen.astype(short.dtype), FLAT).astype(outgoing.dtype)


def dispatch_rows(folded_all, out_weight, table, side_piece, own_cols):
    parts, half, lanes = folded_all.shape
    rows, cols = own_cols.shape
    bf16 = jnp.bfloat16
    whole = pl.BlockSpec(memory_space=pltpu.VMEM)
    return pl.pallas_call(
        dispatch_kernel,
        in_specs=[whole] * 5,
        out_specs=[whole] * 3,
        out_shape=[
            jax.ShapeDtypeStruct((table.shape[0], cols), bf16),
            pltpu.VMEM((rows, cols), jnp.float32),
            pltpu.VMEM((rows, cols), bf16),
        ],
        scratch_shapes=[
            pltpu.VMEM((2, half, parts * lanes), bf16),
            pltpu.VMEM((parts * lanes, cols), bf16),
        ],
        name="dispatch_rows",
        compiler_params=pltpu.CompilerParams(vmem_limit_bytes=GRANT),
    )(*near(folded_all, out_weight, table, side_piece, own_cols))


def pieces_kernel(ready, gate_t, up_t, *refs):
    del ready
    pieces, moved = refs[:-1], refs[-1]
    experts = gate_t.shape[0]
    lane = lax.axis_index("tp_1")
    moves = [
        pltpu.make_async_copy(w.at[(lane + d) % experts], piece.at[i], moved.at[d, i])
        for d, piece in enumerate(pieces)
        for i, w in enumerate((gate_t, up_t))
    ]
    for m in moves:
        m.start()
    for m in moves:
        m.wait()


def expert_pieces(ready, gate_t, up_t):
    experts, units, width = gate_t.shape
    anywhere = pl.BlockSpec(memory_space=pl.ANY)
    whole = pl.BlockSpec(memory_space=pltpu.VMEM)
    return pl.pallas_call(
        pieces_kernel,
        in_specs=[whole] + [anywhere] * 2,
        out_specs=[whole] * experts,
        out_shape=[pltpu.VMEM((2, units, width), gate_t.dtype)] * experts,
        scratch_shapes=[pltpu.SemaphoreType.DMA((experts, 2))],
        name="expert_pieces",
        compiler_params=pltpu.CompilerParams(vmem_limit_bytes=GRANT),
    )(*near(ready), *far(gate_t, up_t))


def mixed_kernel(result, gate_act, message):
    value = result[...]
    scale = lax.rsqrt(jnp.mean(value * value, -1, keepdims=True) + GROUP_EPS)
    mixed = value * scale * jax.nn.silu(gate_act[...])
    half = mixed.shape[0] // 2
    folded = jnp.concatenate([mixed[:half], mixed[half:]], 1)
    message[...] = jnp.broadcast_to(folded[None], message.shape).astype(message.dtype)


def mixed_message(result, gate_act, peers):
    rows, width = result.shape
    whole = pl.BlockSpec(memory_space=pltpu.VMEM)
    return pl.pallas_call(
        mixed_kernel,
        in_specs=[whole] * 2,
        out_specs=whole,
        out_shape=jax.ShapeDtypeStruct((peers, rows // 2, 2 * width), jnp.bfloat16),
        name="mixed_message",
        compiler_params=pltpu.CompilerParams(vmem_limit_bytes=GRANT),
    )(*near(result, gate_act))


def slot_kernel(arrived, own, regroup, message, side, rows, sent):
    experts, row_count, _ = rows.shape
    slots = row_count - own.shape[0]
    span = regroup.shape[1]
    groups = arrived.shape[0] // span
    count = slots // groups
    side_count = side.shape[0] // groups
    for j in range(experts):
        rows[j, slots:] = own[...]
    for g in range(groups):
        moved = f32_dot(regroup[...], arrived[g * span : (g + 1) * span], FLAT).astype(rows.dtype)
        for j in range(experts):
            rows[j, g * count : (g + 1) * count] = moved[j * count : (j + 1) * count]
        side[g * side_count : (g + 1) * side_count] = moved[experts * count :]
    copies = [
        pltpu.make_async_copy(rows, message.at[q], sent.at[q]) for q in range(message.shape[0])
    ]
    for c in copies:
        c.start()
    for c in copies:
        c.wait()


def slot_message(arrived, own, regroup, experts, slots, copies):
    cols = own.shape[1]
    whole = pl.BlockSpec(memory_space=pltpu.VMEM)
    rows = slots + own.shape[0]
    groups = arrived.shape[0] // regroup.shape[1]
    side_rows = regroup.shape[0] * groups - experts * slots
    return pl.pallas_call(
        slot_kernel,
        in_specs=[whole] * 3,
        out_specs=[pl.BlockSpec(memory_space=pl.ANY), whole],
        out_shape=[
            jax.ShapeDtypeStruct((copies, experts, rows, cols), jnp.bfloat16),
            pltpu.VMEM((side_rows, cols), jnp.bfloat16),
        ],
        scratch_shapes=[
            pltpu.VMEM((experts, rows, cols), jnp.bfloat16),
            pltpu.SemaphoreType.DMA((copies,)),
        ],
        name="slot_message",
        compiler_params=pltpu.CompilerParams(vmem_limit_bytes=GRANT),
    )(*near(arrived, own, regroup))


def return_kernel(hidden_all, down, goes, sent_back):
    parts, experts = down.shape[1], down.shape[0]
    span = goes.shape[0]
    groups = sent_back.shape[0] // span
    count = goes.shape[1] // experts
    slots = count * groups
    results = []
    for j in range(experts):
        rows = jnp.concatenate([hidden_all[q * experts + j, :slots] for q in range(parts)], 1)
        mats = jnp.concatenate([down[j, q] for q in range(parts)], 0)
        results.append(f32_dot(rows, mats, FLAT))
    for g in range(groups):
        block = jnp.concatenate([r[g * count : (g + 1) * count] for r in results], 0)
        back = f32_dot(goes[...], block.astype(sent_back.dtype), FLAT)
        sent_back[g * span : (g + 1) * span] = back.astype(sent_back.dtype)


def return_rows(hidden_all, down, goes, groups):
    cols = down.shape[-1]
    whole = pl.BlockSpec(memory_space=pltpu.VMEM)
    return pl.pallas_call(
        return_kernel,
        in_specs=[whole] * 3,
        out_specs=whole,
        out_shape=jax.ShapeDtypeStruct((goes.shape[0] * groups, cols), jnp.bfloat16),
        name="return_rows",
        compiler_params=pltpu.CompilerParams(vmem_limit_bytes=GRANT),
    )(*near(hidden_all, down, goes))


def retain(
    tokens,
    retention_state,
    lengths,
    query_weight,
    key_weight,
    value_weight,
    gate_weight,
    first_head,
):
    row_count = tokens.shape[0]
    head_count = retention_state.shape[1]
    head_width = retention_state.shape[2]

    queries, keys, values, gate_act, positions, own_cols = project_all(
        tokens, lengths, (query_weight, key_weight, value_weight, gate_weight), lax.axis_size(TP)
    )
    by_head = (row_count, head_count, head_width)
    queries = rotate(queries.reshape(by_head), positions)
    key_rows = rotate(keys.reshape(by_head), positions) * head_width ** (-0.5)
    values = values.reshape(by_head)
    head_index = (first_head + jnp.arange(head_count)).astype(jnp.float32)
    decays = 1.0 - 2.0 ** (-5.0 - 7.0 * head_index / (HEADS - 1))
    own_term = jnp.sum(queries * key_rows, -1, keepdims=True) * values
    carried = decays[None, :, None] * jnp.einsum("bhd,bhde->bhe", queries, retention_state)
    result = own_term + carried
    new_state = (
        decays[None, :, None, None] * retention_state
        + key_rows[:, :, :, None] * values[:, :, None, :]
    )
    result = result.reshape(row_count, head_count * head_width)
    return (mixed_message(result, gate_act, lax.axis_size(TP)), new_state, own_cols)


def swap(parts, axis):
    return lax.all_to_all(parts, axis, 0, 0, tiled=True)


def to_all(shard, axis):
    length = lax.axis_size(axis)
    return swap(jnp.broadcast_to(shard[None], (length, *shard.shape)), axis)


def f32_dot(a, b, dims):
    return lax.dot_general(a, b, (dims, ((), ())), preferred_element_type=jnp.float32)


def hidden_kernel(rows_pre, gains, pre_first, own_gain, local_weights, *refs):
    pieces, (message, normed_cols, switch, normed, hidden, gate_up, sent) = refs[:-7], refs[-7:]
    parts, row_count, cols = rows_pre.shape
    own_rows = pre_first.shape[0]
    slots = row_count - own_rows
    width = parts * cols
    total = jnp.zeros((row_count, cols), jnp.float32)
    total_square = jnp.zeros((row_count, cols), jnp.float32)
    for t in range(parts):
        block = rows_pre[t].astype(jnp.float32)
        total = total + block
        total_square = total_square + block * block
    mean = jnp.sum(total, -1, keepdims=True) / width
    square = jnp.sum(total_square, -1, keepdims=True) / width
    scale = lax.rsqrt(square - mean * mean + NORM_EPS)
    for t in range(parts):
        block = (rows_pre[t].astype(jnp.float32) - mean) * scale * gains[t : t + 1]
        normed[:, t * cols : (t + 1) * cols] = block.astype(normed.dtype)
    normed_cols[...] = ((pre_first[...] - mean[slots:]) * scale[slots:] * own_gain[...]).astype(
        normed_cols.dtype
    )
    units = gate_up.shape[0] // 2
    lane = lax.axis_index("tp_1")
    for d, piece in enumerate(pieces):
        span = piece.shape[1]
        start = (lane + len(pieces) - d) % len(pieces) * span
        for i in range(2):
            gate_up[pl.ds(pl.multiple_of(i * units + start, span), span)] = piece[i]
    both = f32_dot(normed[:slots], gate_up[...], ACROSS)
    hidden[:slots] = (jax.nn.silu(both[:, :units]) * both[:, units:]).astype(hidden.dtype)
    local = f32_dot(normed[slots:], local_weights[...], ACROSS)
    cut = (local.shape[1] - RIDER) // 2
    mine = jax.nn.silu(local[:, :cut]) * local[:, cut : 2 * cut]
    mine = jnp.concatenate([mine, jnp.zeros((own_rows, units // 2 - cut), jnp.float32)], 1)
    half = own_rows // 2
    hidden[slots:] = jnp.concatenate([mine[:half], mine[half:]], 1).astype(hidden.dtype)
    copies = [
        pltpu.make_async_copy(hidden, message.at[t], sent.at[t]) for t in range(message.shape[0])
    ]
    for c in copies:
        c.start()
    switch[...] = jax.nn.sigmoid(local[:, 2 * cut : 2 * cut + 1])
    for c in copies:
        c.wait()


def hidden_units(rows_pre, gains, pre_first, own_gain, local_weights, pieces):
    parts, row_count, cols = rows_pre.shape
    units = sum(p.shape[1] for p in pieces)
    own_rows = pre_first.shape[0]
    whole = pl.BlockSpec(memory_space=pltpu.VMEM)
    return pl.pallas_call(
        hidden_kernel,
        in_specs=[whole] * (5 + len(pieces)),
        out_specs=[pl.BlockSpec(memory_space=pl.ANY), whole, whole],
        out_shape=[
            jax.ShapeDtypeStruct((parts, row_count - own_rows // 2, units), jnp.bfloat16),
            pltpu.VMEM((own_rows, cols), jnp.bfloat16),
            pltpu.VMEM((own_rows, 1), jnp.float32),
        ],
        scratch_shapes=[
            pltpu.VMEM((row_count, parts * cols), jnp.bfloat16),
            pltpu.VMEM((row_count - own_rows // 2, units), jnp.bfloat16),
            pltpu.VMEM((2 * units, parts * cols), jnp.bfloat16),
            pltpu.SemaphoreType.DMA((parts,)),
        ],
        name="hidden_units",
        compiler_params=pltpu.CompilerParams(vmem_limit_bytes=GRANT),
    )(*near(rows_pre, gains, pre_first, own_gain, local_weights, *pieces))


def on_device(
    tokens,
    retention_state,
    lengths,
    query_weight,
    key_weight,
    value_weight,
    gate_weight,
    out_weight,
    first_gain,
    routing,
    route_weight,
    expert_gate,
    expert_up,
    expert_down,
    shared_gate,
    shared_up,
    shared_down,
    side_gate,
    side_up,
    side_down,
    side_switch,
    second_gain,
):
    bf16 = jnp.bfloat16
    seq_rows, model_width = tokens.shape
    head_count = retention_state.shape[1]
    col_count = out_weight.shape[1]
    ep_count = lax.axis_size(EP)
    tp_count = lax.axis_size(TP)
    class_count = lax.axis_size("tp_1")
    part_count = lax.axis_size("tp_0")
    local_experts = expert_gate.shape[0]
    hidden_cols = expert_gate.shape[2]
    top_count = routing.shape[1]
    capacity = (3 * seq_rows * top_count + local_experts * ep_count - 1) // (local_experts * ep_count)
    slots = ep_count * capacity
    tp_rank = lax.axis_index(TP)
    col_start = tp_rank * col_count

    folded, new_state, own_cols = retain(
        tokens,
        retention_state,
        lengths,
        query_weight,
        key_weight,
        value_weight,
        gate_weight,
        tp_rank * head_count,
    )
    folded_all = swap(folded, TP)

    same = routing.reshape(-1)[:, None] == routing.reshape(-1)[None, :]
    row_of = jnp.arange(seq_rows * top_count, dtype=jnp.int32) // top_count
    earlier = row_of[None, :] < row_of[:, None]
    position = jnp.sum((same & earlier).astype(jnp.int32), 1).reshape(seq_rows, top_count)
    back_pitch = local_experts * capacity
    out_pitch = back_pitch + RIDER
    place = (routing % local_experts) * capacity + position
    out_ids = (routing // local_experts) * out_pitch + place
    back_ids = (routing // local_experts) * back_pitch + place
    side_cols = side_gate.shape[1]
    side_rows = side_gate.shape[0]
    core_count = lax.axis_size("core")
    wire = jnp.arange(ep_count * out_pitch, dtype=jnp.int32)[:, None]
    chosen = jnp.arange(seq_rows + side_cols, dtype=jnp.int32)[None, :]
    rider_row = (wire // out_pitch) % core_count * RIDER + wire % out_pitch - back_pitch
    table = (wire % out_pitch >= back_pitch) & (chosen == seq_rows + rider_row)
    padded = jnp.pad(out_ids, ((0, side_cols), (0, 0)), constant_values=-1)
    for k in range(top_count):
        table = table | (wire == padded[None, :, k])
    table = table.astype(bf16)
    slot_hot = (
        back_ids.T.reshape(-1)[:, None]
        == jnp.arange(ep_count * back_pitch, dtype=jnp.int32)[None, :]
    ).astype(bf16)

    side_piece = jnp.concatenate([side_gate.T, side_up.T], 1)
    outgoing, pre_first, pre_short = dispatch_rows(
        folded_all,
        out_weight,
        table,
        side_piece,
        own_cols,
    )
    pieces = list(
        expert_pieces(
            pre_short, jnp.swapaxes(expert_gate, 1, 2), jnp.swapaxes(expert_up, 1, 2)
        )
    )
    for d in range(1, class_count):
        steps = [(i, (i + d) % class_count) for i in range(class_count)]
        pieces[d] = lax.ppermute(pieces[d], "tp_1", steps)
    arrived = swap(outgoing.reshape(-1, TILE, col_count), EP).reshape(-1, col_count)

    group_slots = local_experts * GROUP * capacity
    order = jnp.arange(group_slots, dtype=jnp.int32)
    expert, source = order // (GROUP * capacity), order // capacity % GROUP
    spot = expert * capacity + order % capacity
    rider = jnp.arange(GROUP * RIDER, dtype=jnp.int32)
    came_at = jnp.concatenate(
        [source * out_pitch + spot, rider // RIDER * out_pitch + back_pitch + rider % RIDER]
    )
    regroup = (
        came_at[:, None] == jnp.arange(GROUP * out_pitch, dtype=jnp.int32)[None, :]
    ).astype(bf16)
    to_send, side_own = slot_message(
        arrived, pre_short, regroup, local_experts, slots, part_count
    )
    side_own = side_own.reshape(ep_count, RIDER, col_count)
    side_other = lax.ppermute(side_own, "core", [(0, 1), (1, 0)])
    first_core = lax.axis_index("core") == 0
    side_all = jnp.concatenate(
        [
            jnp.where(first_core, side_own, side_other),
            jnp.where(first_core, side_other, side_own),
        ],
        1,
    ).reshape(ep_count, side_cols, 2, side_rows)
    side_all = jnp.transpose(side_all, (2, 1, 0, 3)).reshape(2, side_cols, model_width)
    rows_pre = swap(to_send.reshape(tp_count, slots + seq_rows, col_count), TP)
    own_gain = lax.dynamic_slice_in_dim(first_gain, col_start, col_count, 0)
    units = class_count * hidden_cols
    shared_cols = shared_gate.shape[1]
    local_weights = jnp.concatenate(
        [
            shared_gate.T,
            side_all[0],
            shared_up.T,
            side_all[1],
            jnp.broadcast_to(side_switch[None], (RIDER, model_width)),
        ],
        0,
    )
    hidden, normed_cols, switch = hidden_units(
        rows_pre, first_gain.reshape(tp_count, col_count), pre_first, own_gain[None], local_weights, pieces
    )

    hidden_all = swap(hidden, TP)
    goes_at = source * back_pitch + spot
    goes = (order[:, None] == goes_at[None, :]).astype(bf16)
    down = expert_down.reshape(local_experts, part_count, units, col_count)
    sent_back = return_rows(hidden_all, down, goes, ep_count // GROUP)
    returned = swap(sent_back.reshape(-1, TILE, col_count), EP)

    local_all = hidden_all[:, slots:]
    left = jnp.arange(units, dtype=jnp.int32)[None, None, :] < units // 2
    none = jnp.zeros_like(local_all)
    local_all = in_order(
        jnp.concatenate([jnp.where(left, local_all, none), jnp.where(left, none, local_all)], 1), 1
    )

    def spread(weight, first):
        count = weight.shape[0] // tp_count
        weight = jnp.pad(
            weight.reshape(tp_count, 1, count, col_count),
            ((0, 0), (0, 0), (first, units // 2 - first - count), (0, 0)),
        )
        weight = jnp.broadcast_to(weight, (tp_count, 2, units // 2, col_count))
        return weight.reshape(tp_count * units, col_count)

    shared_out = jnp.dot(
        local_all, spread(shared_down, 0), preferred_element_type=jnp.float32
    )
    side_out = jnp.dot(
        local_all, spread(side_down, shared_cols), preferred_element_type=jnp.float32
    )
    local_sum = (
        RESIDUAL_SCALE * normed_cols.astype(jnp.float32) + shared_out + switch * side_out
    )

    picked = jnp.dot(
        slot_hot, returned.reshape(-1, col_count), preferred_element_type=jnp.float32
    ).reshape(top_count, seq_rows, col_count)
    routed = jnp.sum(picked * route_weight.T[:, :, None], 0)
    pre_second = local_sum + routed
    sums = jnp.stack([jnp.sum(pre_second, -1), jnp.sum(pre_second * pre_second, -1)])
    sums, new_state = lax.optimization_barrier((sums, new_state))
    totals = jnp.sum(to_all(sums, TP), 0)
    mean_second = totals[0][:, None] / model_width
    square_second = totals[1][:, None] / model_width
    output = (
        (pre_second - mean_second)
        * lax.rsqrt(square_second - mean_second * mean_second + NORM_EPS)
        * second_gain
    ).astype(bf16)
    return (output, new_state)


def solution(mesh):
    chips = mesh.devices.reshape(mesh.shape["ep"] // 2, 2, 4, 4)
    finer = Mesh(chips, (*EP, *TP))

    return jax.shard_map(
        on_device,
        mesh=finer,
        in_specs=(
            P(EP, None),
            P(EP, TP, None, None),
            P(EP),
            P(None, TP),
            P(None, TP),
            P(None, TP),
            P(None, TP),
            P(None, TP),
            P(),
            P(EP, None),
            P(EP, None),
            P(EP, None, TP),
            P(EP, None, TP),
            P(EP, None, TP),
            P(None, TP),
            P(None, TP),
            P(None, TP),
            P(EP, TP),
            P(EP, TP),
            P(None, TP),
            P(),
            P(TP),
        ),
        out_specs=(P(EP, TP), P(EP, TP, None, None)),
        check_vma=False,
    )
```

```python
import jax
import jax.numpy as jnp
from jax import lax
from jax.experimental import pallas as pl
from jax.experimental.pallas import tpu as pltpu
from jax.sharding import Mesh
from jax.sharding import PartitionSpec as P

HEADS = 16
TP = ("tp_0", "tp_1")


RESIDUAL_SCALE = 2.0**0.25
NORM_EPS = 1e-05
GROUP_EPS = 1e-06
ROPE_BASE = 10000.0
ACROSS = ((1,), (1,))
EP = ("z", "core")
RIDER = 8
TILE = 4
FLAT = ((1,), (0,))
GROUP = 8
GRANT = 12 * 1024 * 1024


def in_order(parts, dim):
    parts = jnp.moveaxis(parts, 0, dim)
    dims = parts.shape
    return parts.reshape(*dims[:dim], dims[dim] * dims[dim + 1], *dims[dim + 2 :])


def rotate(vector, positions):
    half_width = vector.shape[-1] // 2
    frequency = ROPE_BASE ** (-jnp.arange(half_width, dtype=jnp.float32) / half_width)
    angles = positions[:, None, None] * frequency[None, None, :]
    cosine = jnp.cos(angles)
    sine_part = jnp.sin(angles)
    first_half = vector[..., :half_width]
    second_half = vector[..., half_width:]
    return jnp.concatenate(
        [
            first_half * cosine - second_half * sine_part,
            second_half * cosine + first_half * sine_part,
        ],
        -1,
    )


def near(*arrays):
    return [pltpu.with_memory_space_constraint(a, pltpu.VMEM) for a in arrays]


def far(*arrays):
    return [pltpu.with_memory_space_constraint(a, pltpu.HBM) for a in arrays]


def project_kernel(tokens, lengths, *refs):
    count = (len(refs) - 6) // 2
    weights, outs = refs[:count], refs[count:-6]
    positions, own_cols, rows, held, counts, arrived = refs[-6:]
    cols, width = weights[0].shape
    long = pltpu.make_async_copy(lengths, counts, arrived.at[2, 0])
    span = width // 2
    fetch = []
    for h in range(2):
        at = pl.ds(h * span, span)
        fetch.append(
            [pltpu.make_async_copy(tokens.at[:, at], rows.at[:, at], arrived.at[h, 0])]
            + [
                pltpu.make_async_copy(
                    w.at[:, at], held.at[pl.ds(i * cols, cols), at], arrived.at[h, i + 1]
                )
                for i, w in enumerate(weights)
            ]
        )
        for f in fetch[h]:
            f.start()
    long.start()
    total = None
    for h, group in enumerate(fetch):
        for f in group:
            f.wait()
        at = slice(h * span, (h + 1) * span)
        part = f32_dot(rows[:, at], held[:, at], ACROSS)
        total = part if total is None else total + part
    column = lax.axis_index("tp_0") * lax.axis_size("tp_1") + lax.axis_index("tp_1")
    size = own_cols.shape[1]
    own_cols[...] = rows[:, pl.ds(pl.multiple_of(column * size, size), size)]
    long.wait()
    positions[...] = counts[...].astype(jnp.float32)
    rounded = total.astype(jnp.bfloat16).astype(jnp.float32)
    for i, out in enumerate(outs):
        out[...] = rounded[:, i * cols : (i + 1) * cols]


def project_all(tokens, lengths, weights, parts):
    rows, width = tokens.shape
    cols = weights[0].shape[1]
    count = len(weights)
    anywhere = pl.BlockSpec(memory_space=pl.ANY)
    whole = pl.BlockSpec(memory_space=pltpu.VMEM)
    return pl.pallas_call(
        project_kernel,
        in_specs=[anywhere] * (count + 2),
        out_specs=[whole] * (count + 2),
        out_shape=[pltpu.VMEM((rows, cols), jnp.float32)] * count
        + [
            pltpu.VMEM(lengths.shape, jnp.float32),
            pltpu.VMEM((rows, width // parts), tokens.dtype),
        ],
        scratch_shapes=[
            pltpu.VMEM((rows, width), tokens.dtype),
            pltpu.VMEM((cols * count, width), weights[0].dtype),
            pltpu.VMEM(lengths.shape, lengths.dtype),
            pltpu.SemaphoreType.DMA((3, count + 1)),
        ],
        name="project",
        compiler_params=pltpu.CompilerParams(vmem_limit_bytes=GRANT),
    )(*far(tokens, lengths, *[w.T for w in weights]))


def dispatch_kernel(
    folded_all, out_weight, table, side_piece, own_cols, outgoing, exact, short, lhs, rhs
):
    parts, half, lanes = folded_all.shape
    width = lanes // 2
    lane = lax.broadcasted_iota(jnp.int32, (half, lanes), 1)
    for t in range(parts):
        block = folded_all[t].astype(jnp.float32)
        at = slice(t * lanes, (t + 1) * lanes)
        lhs[0, :, at] = jnp.where(lane < width, block, 0.0).astype(lhs.dtype)
        lhs[1, :, at] = jnp.where(lane < width, 0.0, block).astype(lhs.dtype)
        for i in range(2):
            rhs[t * lanes + i * width : t * lanes + (i + 1) * width] = out_weight[
                t * width : (t + 1) * width
            ]
    mixing = jnp.concatenate([f32_dot(lhs[i], rhs[...], FLAT) for i in range(2)], 0)
    pre_first = RESIDUAL_SCALE * own_cols[...].astype(jnp.float32) + mixing
    exact[...] = pre_first
    pre_short = pre_first.astype(short.dtype)
    short[...] = pre_short
    chosen = jnp.concatenate([pre_first, side_piece[...].astype(jnp.float32)], 0)
    outgoing[...] = f32_dot(table[...], chosen.astype(short.dtype), FLAT).astype(outgoing.dtype)


def dispatch_rows(folded_all, out_weight, table, side_piece, own_cols):
    parts, half, lanes = folded_all.shape
    rows, cols = own_cols.shape
    bf16 = jnp.bfloat16
    whole = pl.BlockSpec(memory_space=pltpu.VMEM)
    return pl.pallas_call(
        dispatch_kernel,
        in_specs=[whole] * 5,
        out_specs=[whole] * 3,
        out_shape=[
            jax.ShapeDtypeStruct((table.shape[0], cols), bf16),
            pltpu.VMEM((rows, cols), jnp.float32),
            pltpu.VMEM((rows, cols), bf16),
        ],
        scratch_shapes=[
            pltpu.VMEM((2, half, parts * lanes), bf16),
            pltpu.VMEM((parts * lanes, cols), bf16),
        ],
        name="dispatch_rows",
        compiler_params=pltpu.CompilerParams(vmem_limit_bytes=GRANT),
    )(*near(folded_all, out_weight, table, side_piece, own_cols))


def pieces_kernel(ready, gate_t, up_t, *refs):
    del ready
    pieces, moved = refs[:-1], refs[-1]
    experts = gate_t.shape[0]
    lane = lax.axis_index("tp_1")
    moves = [
        pltpu.make_async_copy(w.at[(lane + d) % experts], piece.at[i], moved.at[d, i])
        for d, piece in enumerate(pieces)
        for i, w in enumerate((gate_t, up_t))
    ]
    for m in moves:
        m.start()
    for m in moves:
        m.wait()


def expert_pieces(ready, gate_t, up_t):
    experts, units, width = gate_t.shape
    anywhere = pl.BlockSpec(memory_space=pl.ANY)
    whole = pl.BlockSpec(memory_space=pltpu.VMEM)
    return pl.pallas_call(
        pieces_kernel,
        in_specs=[whole] + [anywhere] * 2,
        out_specs=[whole] * experts,
        out_shape=[pltpu.VMEM((2, units, width), gate_t.dtype)] * experts,
        scratch_shapes=[pltpu.SemaphoreType.DMA((experts, 2))],
        name="expert_pieces",
        compiler_params=pltpu.CompilerParams(vmem_limit_bytes=GRANT),
    )(*near(ready), *far(gate_t, up_t))


def mixed_kernel(result, gate_act, message):
    value = result[...]
    scale = lax.rsqrt(jnp.mean(value * value, -1, keepdims=True) + GROUP_EPS)
    mixed = value * scale * jax.nn.silu(gate_act[...])
    half = mixed.shape[0] // 2
    folded = jnp.concatenate([mixed[:half], mixed[half:]], 1)
    message[...] = jnp.broadcast_to(folded[None], message.shape).astype(message.dtype)


def mixed_message(result, gate_act, peers):
    rows, width = result.shape
    whole = pl.BlockSpec(memory_space=pltpu.VMEM)
    return pl.pallas_call(
        mixed_kernel,
        in_specs=[whole] * 2,
        out_specs=whole,
        out_shape=jax.ShapeDtypeStruct((peers, rows // 2, 2 * width), jnp.bfloat16),
        name="mixed_message",
        compiler_params=pltpu.CompilerParams(vmem_limit_bytes=GRANT),
    )(*near(result, gate_act))


def slot_kernel(arrived, own, regroup, message, side, rows, sent):
    experts, row_count, _ = rows.shape
    slots = row_count - own.shape[0]
    span = regroup.shape[1]
    groups = arrived.shape[0] // span
    count = slots // groups
    side_count = side.shape[0] // groups
    for j in range(experts):
        rows[j, slots:] = own[...]
    for g in range(groups):
        moved = f32_dot(regroup[...], arrived[g * span : (g + 1) * span], FLAT).astype(rows.dtype)
        for j in range(experts):
            rows[j, g * count : (g + 1) * count] = moved[j * count : (j + 1) * count]
        side[g * side_count : (g + 1) * side_count] = moved[experts * count :]
    copies = [
        pltpu.make_async_copy(rows, message.at[q], sent.at[q]) for q in range(message.shape[0])
    ]
    for c in copies:
        c.start()
    for c in copies:
        c.wait()


def slot_message(arrived, own, regroup, experts, slots, copies):
    cols = own.shape[1]
    whole = pl.BlockSpec(memory_space=pltpu.VMEM)
    rows = slots + own.shape[0]
    groups = arrived.shape[0] // regroup.shape[1]
    side_rows = regroup.shape[0] * groups - experts * slots
    return pl.pallas_call(
        slot_kernel,
        in_specs=[whole] * 3,
        out_specs=[pl.BlockSpec(memory_space=pl.ANY), whole],
        out_shape=[
            jax.ShapeDtypeStruct((copies, experts, rows, cols), jnp.bfloat16),
            pltpu.VMEM((side_rows, cols), jnp.bfloat16),
        ],
        scratch_shapes=[
            pltpu.VMEM((experts, rows, cols), jnp.bfloat16),
            pltpu.SemaphoreType.DMA((copies,)),
        ],
        name="slot_message",
        compiler_params=pltpu.CompilerParams(vmem_limit_bytes=GRANT),
    )(*near(arrived, own, regroup))


def return_kernel(hidden_all, down, goes, sent_back):
    parts, experts = down.shape[1], down.shape[0]
    span = goes.shape[0]
    groups = sent_back.shape[0] // span
    count = goes.shape[1] // experts
    slots = count * groups
    results = []
    for j in range(experts):
        rows = jnp.concatenate([hidden_all[q * experts + j, :slots] for q in range(parts)], 1)
        mats = jnp.concatenate([down[j, q] for q in range(parts)], 0)
        results.append(f32_dot(rows, mats, FLAT))
    for g in range(groups):
        block = jnp.concatenate([r[g * count : (g + 1) * count] for r in results], 0)
        back = f32_dot(goes[...], block.astype(sent_back.dtype), FLAT)
        sent_back[g * span : (g + 1) * span] = back.astype(sent_back.dtype)


def return_rows(hidden_all, down, goes, groups):
    cols = down.shape[-1]
    whole = pl.BlockSpec(memory_space=pltpu.VMEM)
    return pl.pallas_call(
        return_kernel,
        in_specs=[whole] * 3,
        out_specs=whole,
        out_shape=jax.ShapeDtypeStruct((goes.shape[0] * groups, cols), jnp.bfloat16),
        name="return_rows",
        compiler_params=pltpu.CompilerParams(vmem_limit_bytes=GRANT),
    )(*near(hidden_all, down, goes))


def retain(
    tokens,
    retention_state,
    lengths,
    query_weight,
    key_weight,
    value_weight,
    gate_weight,
    first_head,
):
    row_count = tokens.shape[0]
    head_count = retention_state.shape[1]
    head_width = retention_state.shape[2]

    queries, keys, values, gate_act, positions, own_cols = project_all(
        tokens, lengths, (query_weight, key_weight, value_weight, gate_weight), lax.axis_size(TP)
    )
    by_head = (row_count, head_count, head_width)
    queries = rotate(queries.reshape(by_head), positions)
    key_rows = rotate(keys.reshape(by_head), positions) * head_width ** (-0.5)
    values = values.reshape(by_head)
    head_index = (first_head + jnp.arange(head_count)).astype(jnp.float32)
    decays = 1.0 - 2.0 ** (-5.0 - 7.0 * head_index / (HEADS - 1))
    own_term = jnp.sum(queries * key_rows, -1, keepdims=True) * values
    carried = decays[None, :, None] * jnp.einsum("bhd,bhde->bhe", queries, retention_state)
    result = own_term + carried
    new_state = (
        decays[None, :, None, None] * retention_state
        + key_rows[:, :, :, None] * values[:, :, None, :]
    )
    result = result.reshape(row_count, head_count * head_width)
    return (mixed_message(result, gate_act, lax.axis_size(TP)), new_state, own_cols)


def swap(parts, axis):
    return lax.all_to_all(parts, axis, 0, 0, tiled=True)


def to_all(shard, axis):
    length = lax.axis_size(axis)
    return swap(jnp.broadcast_to(shard[None], (length, *shard.shape)), axis)


def f32_dot(a, b, dims):
    return lax.dot_general(a, b, (dims, ((), ())), preferred_element_type=jnp.float32)


def ordered_kernel(*refs):
    pieces, gate_up = refs[:-1], refs[-1]
    units = gate_up.shape[0] // 2
    lane = lax.axis_index("tp_1")
    for d, piece in enumerate(pieces):
        span = piece.shape[1]
        start = (lane + len(pieces) - d) % len(pieces) * span
        for i in range(2):
            gate_up[pl.ds(pl.multiple_of(i * units + start, span), span)] = piece[i]


def ordered(pieces):
    two, span, width = pieces[0].shape
    whole = pl.BlockSpec(memory_space=pltpu.VMEM)
    return pl.pallas_call(
        ordered_kernel,
        in_specs=[whole] * len(pieces),
        out_specs=whole,
        out_shape=pltpu.VMEM((two * span * len(pieces), width), pieces[0].dtype),
        name="ordered",
        compiler_params=pltpu.CompilerParams(vmem_limit_bytes=GRANT),
    )(*near(*pieces))


def hidden_kernel(
    rows_pre, gains, pre_first, own_gain, local_weights, gate_up, message, normed_cols, switch, normed
):
    parts, row_count, cols = rows_pre.shape
    own_rows = pre_first.shape[0]
    slots = row_count - own_rows
    width = parts * cols
    total = jnp.zeros((row_count, cols), jnp.float32)
    total_square = jnp.zeros((row_count, cols), jnp.float32)
    for t in range(parts):
        block = rows_pre[t].astype(jnp.float32)
        total = total + block
        total_square = total_square + block * block
    mean = jnp.sum(total, -1, keepdims=True) / width
    square = jnp.sum(total_square, -1, keepdims=True) / width
    scale = lax.rsqrt(square - mean * mean + NORM_EPS)
    for t in range(parts):
        block = (rows_pre[t].astype(jnp.float32) - mean) * scale * gains[t : t + 1]
        normed[:, t * cols : (t + 1) * cols] = block.astype(normed.dtype)
    normed_cols[...] = ((pre_first[...] - mean[slots:]) * scale[slots:] * own_gain[...]).astype(
        normed_cols.dtype
    )
    units = gate_up.shape[0] // 2
    both = f32_dot(normed[:slots], gate_up[...], ACROSS)
    routed = (jax.nn.silu(both[:, :units]) * both[:, units:]).astype(message.dtype)
    for t in range(message.shape[0]):
        message[t, :slots] = routed
    local = f32_dot(normed[slots:], local_weights[...], ACROSS)
    cut = (local.shape[1] - RIDER) // 2
    mine = jax.nn.silu(local[:, :cut]) * local[:, cut : 2 * cut]
    mine = jnp.concatenate([mine, jnp.zeros((own_rows, units // 2 - cut), jnp.float32)], 1)
    half = own_rows // 2
    packed = jnp.concatenate([mine[:half], mine[half:]], 1).astype(message.dtype)
    for t in range(message.shape[0]):
        message[t, slots:] = packed
    switch[...] = jax.nn.sigmoid(local[:, 2 * cut : 2 * cut + 1])


def hidden_units(rows_pre, gains, pre_first, own_gain, local_weights, gate_up):
    parts, row_count, cols = rows_pre.shape
    units = gate_up.shape[0] // 2
    own_rows = pre_first.shape[0]
    whole = pl.BlockSpec(memory_space=pltpu.VMEM)
    return pl.pallas_call(
        hidden_kernel,
        in_specs=[whole] * 6,
        out_specs=[whole] * 3,
        out_shape=[
            jax.ShapeDtypeStruct((parts, row_count - own_rows // 2, units), jnp.bfloat16),
            pltpu.VMEM((own_rows, cols), jnp.bfloat16),
            pltpu.VMEM((own_rows, 1), jnp.float32),
        ],
        scratch_shapes=[pltpu.VMEM((row_count, parts * cols), jnp.bfloat16)],
        name="hidden_units",
        compiler_params=pltpu.CompilerParams(vmem_limit_bytes=GRANT),
    )(*near(rows_pre, gains, pre_first, own_gain, local_weights, gate_up))


def on_device(
    tokens,
    retention_state,
    lengths,
    query_weight,
    key_weight,
    value_weight,
    gate_weight,
    out_weight,
    first_gain,
    routing,
    route_weight,
    expert_gate,
    expert_up,
    expert_down,
    shared_gate,
    shared_up,
    shared_down,
    side_gate,
    side_up,
    side_down,
    side_switch,
    second_gain,
):
    bf16 = jnp.bfloat16
    seq_rows, model_width = tokens.shape
    head_count = retention_state.shape[1]
    col_count = out_weight.shape[1]
    ep_count = lax.axis_size(EP)
    tp_count = lax.axis_size(TP)
    class_count = lax.axis_size("tp_1")
    part_count = lax.axis_size("tp_0")
    local_experts = expert_gate.shape[0]
    hidden_cols = expert_gate.shape[2]
    top_count = routing.shape[1]
    capacity = (3 * seq_rows * top_count + local_experts * ep_count - 1) // (local_experts * ep_count)
    slots = ep_count * capacity
    tp_rank = lax.axis_index(TP)
    col_start = tp_rank * col_count

    folded, new_state, own_cols = retain(
        tokens,
        retention_state,
        lengths,
        query_weight,
        key_weight,
        value_weight,
        gate_weight,
        tp_rank * head_count,
    )
    folded_all = swap(folded, TP)

    same = routing.reshape(-1)[:, None] == routing.reshape(-1)[None, :]
    row_of = jnp.arange(seq_rows * top_count, dtype=jnp.int32) // top_count
    earlier = row_of[None, :] < row_of[:, None]
    position = jnp.sum((same & earlier).astype(jnp.int32), 1).reshape(seq_rows, top_count)
    back_pitch = local_experts * capacity
    out_pitch = back_pitch + RIDER
    place = (routing % local_experts) * capacity + position
    out_ids = (routing // local_experts) * out_pitch + place
    back_ids = (routing // local_experts) * back_pitch + place
    side_cols = side_gate.shape[1]
    side_rows = side_gate.shape[0]
    core_count = lax.axis_size("core")
    wire = jnp.arange(ep_count * out_pitch, dtype=jnp.int32)[:, None]
    chosen = jnp.arange(seq_rows + side_cols, dtype=jnp.int32)[None, :]
    rider_row = (wire // out_pitch) % core_count * RIDER + wire % out_pitch - back_pitch
    table = (wire % out_pitch >= back_pitch) & (chosen == seq_rows + rider_row)
    padded = jnp.pad(out_ids, ((0, side_cols), (0, 0)), constant_values=-1)
    for k in range(top_count):
        table = table | (wire == padded[None, :, k])
    table = table.astype(bf16)
    slot_hot = (
        back_ids.T.reshape(-1)[:, None]
        == jnp.arange(ep_count * back_pitch, dtype=jnp.int32)[None, :]
    ).astype(bf16)

    side_piece = jnp.concatenate([side_gate.T, side_up.T], 1)
    outgoing, pre_first, pre_short = dispatch_rows(
        folded_all,
        out_weight,
        table,
        side_piece,
        own_cols,
    )
    pieces = list(
        expert_pieces(
            pre_short, jnp.swapaxes(expert_gate, 1, 2), jnp.swapaxes(expert_up, 1, 2)
        )
    )
    for d in sorted(range(1, class_count), key=lambda d: -min(d, class_count - d)):
        steps = [(i, (i + d) % class_count) for i in range(class_count)]
        pieces[d] = lax.ppermute(pieces[d], "tp_1", steps)
    arrived = swap(outgoing.reshape(-1, TILE, col_count), EP).reshape(-1, col_count)

    group_slots = local_experts * GROUP * capacity
    order = jnp.arange(group_slots, dtype=jnp.int32)
    expert, source = order // (GROUP * capacity), order // capacity % GROUP
    spot = expert * capacity + order % capacity
    rider = jnp.arange(GROUP * RIDER, dtype=jnp.int32)
    came_at = jnp.concatenate(
        [source * out_pitch + spot, rider // RIDER * out_pitch + back_pitch + rider % RIDER]
    )
    regroup = (
        came_at[:, None] == jnp.arange(GROUP * out_pitch, dtype=jnp.int32)[None, :]
    ).astype(bf16)
    to_send, side_own = slot_message(
        arrived, pre_short, regroup, local_experts, slots, part_count
    )
    side_own = side_own.reshape(ep_count, RIDER, col_count)
    side_other = lax.ppermute(side_own, "core", [(0, 1), (1, 0)])
    first_core = lax.axis_index("core") == 0
    side_all = jnp.concatenate(
        [
            jnp.where(first_core, side_own, side_other),
            jnp.where(first_core, side_other, side_own),
        ],
        1,
    ).reshape(ep_count, side_cols, 2, side_rows)
    side_all = jnp.transpose(side_all, (2, 1, 0, 3)).reshape(2, side_cols, model_width)
    rows_pre = swap(to_send.reshape(tp_count, slots + seq_rows, col_count), TP)
    own_gain = lax.dynamic_slice_in_dim(first_gain, col_start, col_count, 0)
    units = class_count * hidden_cols
    shared_cols = shared_gate.shape[1]
    local_weights = jnp.concatenate(
        [
            shared_gate.T,
            side_all[0],
            shared_up.T,
            side_all[1],
            jnp.broadcast_to(side_switch[None], (RIDER, model_width)),
        ],
        0,
    )
    hidden, normed_cols, switch = hidden_units(
        rows_pre, first_gain.reshape(tp_count, col_count), pre_first, own_gain[None], local_weights, ordered(pieces)
    )

    hidden_all = swap(hidden, TP)
    goes_at = source * back_pitch + spot
    goes = (order[:, None] == goes_at[None, :]).astype(bf16)
    down = expert_down.reshape(local_experts, part_count, units, col_count)
    sent_back = return_rows(hidden_all, down, goes, ep_count // GROUP)
    returned = swap(sent_back.reshape(-1, TILE, col_count), EP)

    local_all = hidden_all[:, slots:]
    left = jnp.arange(units, dtype=jnp.int32)[None, None, :] < units // 2
    none = jnp.zeros_like(local_all)
    local_all = in_order(
        jnp.concatenate([jnp.where(left, local_all, none), jnp.where(left, none, local_all)], 1), 1
    )

    def spread(weight, first):
        count = weight.shape[0] // tp_count
        weight = jnp.pad(
            weight.reshape(tp_count, 1, count, col_count),
            ((0, 0), (0, 0), (first, units // 2 - first - count), (0, 0)),
        )
        weight = jnp.broadcast_to(weight, (tp_count, 2, units // 2, col_count))
        return weight.reshape(tp_count * units, col_count)

    shared_out = jnp.dot(
        local_all, spread(shared_down, 0), preferred_element_type=jnp.float32
    )
    side_out = jnp.dot(
        local_all, spread(side_down, shared_cols), preferred_element_type=jnp.float32
    )
    local_sum = (
        RESIDUAL_SCALE * normed_cols.astype(jnp.float32) + shared_out + switch * side_out
    )

    picked = jnp.dot(
        slot_hot, returned.reshape(-1, col_count), preferred_element_type=jnp.float32
    ).reshape(top_count, seq_rows, col_count)
    routed = jnp.sum(picked * route_weight.T[:, :, None], 0)
    pre_second = local_sum + routed
    sums = jnp.stack([jnp.sum(pre_second, -1), jnp.sum(pre_second * pre_second, -1)])
    sums, new_state = lax.optimization_barrier((sums, new_state))
    totals = jnp.sum(to_all(sums, TP), 0)
    mean_second = totals[0][:, None] / model_width
    square_second = totals[1][:, None] / model_width
    output = (
        (pre_second - mean_second)
        * lax.rsqrt(square_second - mean_second * mean_second + NORM_EPS)
        * second_gain
    ).astype(bf16)
    return (output, new_state)


def solution(mesh):
    chips = mesh.devices.reshape(mesh.shape["ep"] // 2, 2, 4, 4)
    finer = Mesh(chips, (*EP, *TP))

    return jax.shard_map(
        on_device,
        mesh=finer,
        in_specs=(
            P(EP, None),
            P(EP, TP, None, None),
            P(EP),
            P(None, TP),
            P(None, TP),
            P(None, TP),
            P(None, TP),
            P(None, TP),
            P(),
            P(EP, None),
            P(EP, None),
            P(EP, None, TP),
            P(EP, None, TP),
            P(EP, None, TP),
            P(None, TP),
            P(None, TP),
            P(None, TP),
            P(EP, TP),
            P(EP, TP),
            P(None, TP),
            P(),
            P(TP),
        ),
        out_specs=(P(EP, TP), P(EP, TP, None, None)),
        check_vma=False,
    )
```

```python
import jax
import jax.numpy as jnp
from jax import lax
from jax.experimental import pallas as pl
from jax.experimental.pallas import tpu as pltpu
from jax.sharding import Mesh
from jax.sharding import PartitionSpec as P

HEADS = 16
TP = ("tp_0", "tp_1")


RESIDUAL_SCALE = 2.0**0.25
NORM_EPS = 1e-05
GROUP_EPS = 1e-06
ROPE_BASE = 10000.0
ACROSS = ((1,), (1,))
EP = ("z", "core")
RIDER = 8
TILE = 4
FLAT = ((1,), (0,))
GROUP = 8
GRANT = 12 * 1024 * 1024


def in_order(parts, dim):
    parts = jnp.moveaxis(parts, 0, dim)
    dims = parts.shape
    return parts.reshape(*dims[:dim], dims[dim] * dims[dim + 1], *dims[dim + 2 :])


def rotate(vector, positions):
    half_width = vector.shape[-1] // 2
    frequency = ROPE_BASE ** (-jnp.arange(half_width, dtype=jnp.float32) / half_width)
    angles = positions[:, None, None] * frequency[None, None, :]
    cosine = jnp.cos(angles)
    sine_part = jnp.sin(angles)
    first_half = vector[..., :half_width]
    second_half = vector[..., half_width:]
    return jnp.concatenate(
        [
            first_half * cosine - second_half * sine_part,
            second_half * cosine + first_half * sine_part,
        ],
        -1,
    )


def near(*arrays):
    return [pltpu.with_memory_space_constraint(a, pltpu.VMEM) for a in arrays]


def far(*arrays):
    return [pltpu.with_memory_space_constraint(a, pltpu.HBM) for a in arrays]


def project_kernel(tokens, lengths, *refs):
    count = (len(refs) - 6) // 2
    weights, outs = refs[:count], refs[count:-6]
    positions, own_cols, rows, held, counts, arrived = refs[-6:]
    cols, width = weights[0].shape
    long = pltpu.make_async_copy(lengths, counts, arrived.at[2, 0])
    span = width // 2
    fetch = []
    for h in range(2):
        at = pl.ds(h * span, span)
        fetch.append(
            [pltpu.make_async_copy(tokens.at[:, at], rows.at[:, at], arrived.at[h, 0])]
            + [
                pltpu.make_async_copy(
                    w.at[:, at], held.at[pl.ds(i * cols, cols), at], arrived.at[h, i + 1]
                )
                for i, w in enumerate(weights)
            ]
        )
        for f in fetch[h]:
            f.start()
    long.start()
    total = None
    for h, group in enumerate(fetch):
        for f in group:
            f.wait()
        at = slice(h * span, (h + 1) * span)
        part = f32_dot(rows[:, at], held[:, at], ACROSS)
        total = part if total is None else total + part
    column = lax.axis_index("tp_0") * lax.axis_size("tp_1") + lax.axis_index("tp_1")
    size = own_cols.shape[1]
    own_cols[...] = rows[:, pl.ds(pl.multiple_of(column * size, size), size)]
    long.wait()
    positions[...] = counts[...].astype(jnp.float32)
    rounded = total.astype(jnp.bfloat16).astype(jnp.float32)
    for i, out in enumerate(outs):
        out[...] = rounded[:, i * cols : (i + 1) * cols]


def project_all(tokens, lengths, weights, parts):
    rows, width = tokens.shape
    cols = weights[0].shape[1]
    count = len(weights)
    anywhere = pl.BlockSpec(memory_space=pl.ANY)
    whole = pl.BlockSpec(memory_space=pltpu.VMEM)
    return pl.pallas_call(
        project_kernel,
        in_specs=[anywhere] * (count + 2),
        out_specs=[whole] * (count + 2),
        out_shape=[pltpu.VMEM((rows, cols), jnp.float32)] * count
        + [
            pltpu.VMEM(lengths.shape, jnp.float32),
            pltpu.VMEM((rows, width // parts), tokens.dtype),
        ],
        scratch_shapes=[
            pltpu.VMEM((rows, width), tokens.dtype),
            pltpu.VMEM((cols * count, width), weights[0].dtype),
            pltpu.VMEM(lengths.shape, lengths.dtype),
            pltpu.SemaphoreType.DMA((3, count + 1)),
        ],
        name="project",
        compiler_params=pltpu.CompilerParams(vmem_limit_bytes=GRANT),
    )(*far(tokens, lengths, *[w.T for w in weights]))


def dispatch_kernel(
    folded_all, out_weight, table, side_piece, own_cols, outgoing, exact, short, lhs
):
    parts, half, lanes = folded_all.shape
    width = lanes // 2
    lane = lax.broadcasted_iota(jnp.int32, (half, lanes), 1)
    for t in range(parts):
        block = folded_all[t].astype(jnp.float32)
        at = slice(t * lanes, (t + 1) * lanes)
        lhs[0, :, at] = jnp.where(lane < width, block, 0.0).astype(lhs.dtype)
        lhs[1, :, at] = jnp.where(lane < width, 0.0, block).astype(lhs.dtype)
    mixing = jnp.concatenate([f32_dot(lhs[i], out_weight[...], FLAT) for i in range(2)], 0)
    pre_first = RESIDUAL_SCALE * own_cols[...].astype(jnp.float32) + mixing
    exact[...] = pre_first
    pre_short = pre_first.astype(short.dtype)
    short[...] = pre_short
    chosen = jnp.concatenate([pre_first, side_piece[...].astype(jnp.float32)], 0)
    outgoing[...] = f32_dot(table[...], chosen.astype(short.dtype), FLAT).astype(outgoing.dtype)


def dispatch_rows(folded_all, out_weight, table, side_piece, own_cols):
    parts, half, lanes = folded_all.shape
    rows, cols = own_cols.shape
    bf16 = jnp.bfloat16
    whole = pl.BlockSpec(memory_space=pltpu.VMEM)
    return pl.pallas_call(
        dispatch_kernel,
        in_specs=[whole] * 5,
        out_specs=[whole] * 3,
        out_shape=[
            jax.ShapeDtypeStruct((table.shape[0], cols), bf16),
            pltpu.VMEM((rows, cols), jnp.float32),
            pltpu.VMEM((rows, cols), bf16),
        ],
        scratch_shapes=[
            pltpu.VMEM((2, half, parts * lanes), bf16),
        ],
        name="dispatch_rows",
        compiler_params=pltpu.CompilerParams(vmem_limit_bytes=GRANT),
    )(*near(folded_all, out_weight, table, side_piece, own_cols))


def pieces_kernel(ready, gate_t, up_t, *refs):
    del ready
    pieces, moved = refs[:-1], refs[-1]
    experts = gate_t.shape[0]
    lane = lax.axis_index("tp_1")
    moves = [
        pltpu.make_async_copy(w.at[(lane + d) % experts], piece.at[i], moved.at[d, i])
        for d, piece in enumerate(pieces)
        for i, w in enumerate((gate_t, up_t))
    ]
    for m in moves:
        m.start()
    for m in moves:
        m.wait()


def expert_pieces(ready, gate_t, up_t):
    experts, units, width = gate_t.shape
    anywhere = pl.BlockSpec(memory_space=pl.ANY)
    whole = pl.BlockSpec(memory_space=pltpu.VMEM)
    return pl.pallas_call(
        pieces_kernel,
        in_specs=[whole] + [anywhere] * 2,
        out_specs=[whole] * experts,
        out_shape=[pltpu.VMEM((2, units, width), gate_t.dtype)] * experts,
        scratch_shapes=[pltpu.SemaphoreType.DMA((experts, 2))],
        name="expert_pieces",
        compiler_params=pltpu.CompilerParams(vmem_limit_bytes=GRANT),
    )(*near(ready), *far(gate_t, up_t))


def mixed_kernel(result, gate_act, message):
    value = result[...]
    scale = lax.rsqrt(jnp.mean(value * value, -1, keepdims=True) + GROUP_EPS)
    mixed = value * scale * jax.nn.silu(gate_act[...])
    half = mixed.shape[0] // 2
    folded = jnp.concatenate([mixed[:half], mixed[half:]], 1)
    message[...] = jnp.broadcast_to(folded[None], message.shape).astype(message.dtype)


def mixed_message(result, gate_act, peers):
    rows, width = result.shape
    whole = pl.BlockSpec(memory_space=pltpu.VMEM)
    return pl.pallas_call(
        mixed_kernel,
        in_specs=[whole] * 2,
        out_specs=whole,
        out_shape=jax.ShapeDtypeStruct((peers, rows // 2, 2 * width), jnp.bfloat16),
        name="mixed_message",
        compiler_params=pltpu.CompilerParams(vmem_limit_bytes=GRANT),
    )(*near(result, gate_act))


def slot_kernel(arrived, own, regroup, message, side, rows, sent):
    experts, row_count, _ = rows.shape
    slots = row_count - own.shape[0]
    span = regroup.shape[1]
    groups = arrived.shape[0] // span
    count = slots // groups
    side_count = side.shape[0] // groups
    for j in range(experts):
        rows[j, slots:] = own[...]
    for g in range(groups):
        moved = f32_dot(regroup[...], arrived[g * span : (g + 1) * span], FLAT).astype(rows.dtype)
        for j in range(experts):
            rows[j, g * count : (g + 1) * count] = moved[j * count : (j + 1) * count]
        side[g * side_count : (g + 1) * side_count] = moved[experts * count :]
    copies = [
        pltpu.make_async_copy(rows, message.at[q], sent.at[q]) for q in range(message.shape[0])
    ]
    for c in copies:
        c.start()
    for c in copies:
        c.wait()


def slot_message(arrived, own, regroup, experts, slots, copies):
    cols = own.shape[1]
    whole = pl.BlockSpec(memory_space=pltpu.VMEM)
    rows = slots + own.shape[0]
    groups = arrived.shape[0] // regroup.shape[1]
    side_rows = regroup.shape[0] * groups - experts * slots
    return pl.pallas_call(
        slot_kernel,
        in_specs=[whole] * 3,
        out_specs=[pl.BlockSpec(memory_space=pl.ANY), whole],
        out_shape=[
            jax.ShapeDtypeStruct((copies, experts, rows, cols), jnp.bfloat16),
            pltpu.VMEM((side_rows, cols), jnp.bfloat16),
        ],
        scratch_shapes=[
            pltpu.VMEM((experts, rows, cols), jnp.bfloat16),
            pltpu.SemaphoreType.DMA((copies,)),
        ],
        name="slot_message",
        compiler_params=pltpu.CompilerParams(vmem_limit_bytes=GRANT),
    )(*near(arrived, own, regroup))


def return_kernel(hidden_all, down, goes, sent_back):
    parts, experts = down.shape[1], down.shape[0]
    span = goes.shape[0]
    groups = sent_back.shape[0] // span
    count = goes.shape[1] // experts
    slots = count * groups
    results = []
    for j in range(experts):
        rows = jnp.concatenate([hidden_all[q * experts + j, :slots] for q in range(parts)], 1)
        mats = jnp.concatenate([down[j, q] for q in range(parts)], 0)
        results.append(f32_dot(rows, mats, FLAT))
    for g in range(groups):
        block = jnp.concatenate([r[g * count : (g + 1) * count] for r in results], 0)
        back = f32_dot(goes[...], block.astype(sent_back.dtype), FLAT)
        sent_back[g * span : (g + 1) * span] = back.astype(sent_back.dtype)


def return_rows(hidden_all, down, goes, groups):
    cols = down.shape[-1]
    whole = pl.BlockSpec(memory_space=pltpu.VMEM)
    return pl.pallas_call(
        return_kernel,
        in_specs=[whole] * 3,
        out_specs=whole,
        out_shape=jax.ShapeDtypeStruct((goes.shape[0] * groups, cols), jnp.bfloat16),
        name="return_rows",
        compiler_params=pltpu.CompilerParams(vmem_limit_bytes=GRANT),
    )(*near(hidden_all, down, goes))


def retain(
    tokens,
    retention_state,
    lengths,
    query_weight,
    key_weight,
    value_weight,
    gate_weight,
    first_head,
):
    row_count = tokens.shape[0]
    head_count = retention_state.shape[1]
    head_width = retention_state.shape[2]

    queries, keys, values, gate_act, positions, own_cols = project_all(
        tokens, lengths, (query_weight, key_weight, value_weight, gate_weight), lax.axis_size(TP)
    )
    by_head = (row_count, head_count, head_width)
    queries = rotate(queries.reshape(by_head), positions)
    key_rows = rotate(keys.reshape(by_head), positions) * head_width ** (-0.5)
    values = values.reshape(by_head)
    head_index = (first_head + jnp.arange(head_count)).astype(jnp.float32)
    decays = 1.0 - 2.0 ** (-5.0 - 7.0 * head_index / (HEADS - 1))
    own_term = jnp.sum(queries * key_rows, -1, keepdims=True) * values
    carried = decays[None, :, None] * jnp.einsum("bhd,bhde->bhe", queries, retention_state)
    result = own_term + carried
    new_state = (
        decays[None, :, None, None] * retention_state
        + key_rows[:, :, :, None] * values[:, :, None, :]
    )
    result = result.reshape(row_count, head_count * head_width)
    return (mixed_message(result, gate_act, lax.axis_size(TP)), new_state, own_cols)


def swap(parts, axis):
    return lax.all_to_all(parts, axis, 0, 0, tiled=True)


def to_all(shard, axis):
    length = lax.axis_size(axis)
    return swap(jnp.broadcast_to(shard[None], (length, *shard.shape)), axis)


def f32_dot(a, b, dims):
    return lax.dot_general(a, b, (dims, ((), ())), preferred_element_type=jnp.float32)


def ordered_kernel(*refs):
    pieces, gate_up = refs[:-1], refs[-1]
    units = gate_up.shape[0] // 2
    lane = lax.axis_index("tp_1")
    for d, piece in enumerate(pieces):
        span = piece.shape[1]
        start = (lane + len(pieces) - d) % len(pieces) * span
        for i in range(2):
            gate_up[pl.ds(pl.multiple_of(i * units + start, span), span)] = piece[i]


def ordered(pieces):
    two, span, width = pieces[0].shape
    whole = pl.BlockSpec(memory_space=pltpu.VMEM)
    return pl.pallas_call(
        ordered_kernel,
        in_specs=[whole] * len(pieces),
        out_specs=whole,
        out_shape=pltpu.VMEM((two * span * len(pieces), width), pieces[0].dtype),
        name="ordered",
        compiler_params=pltpu.CompilerParams(vmem_limit_bytes=GRANT),
    )(*near(*pieces))


def hidden_kernel(
    rows_pre, gains, pre_first, own_gain, local_weights, gate_up, message, normed_cols, switch, normed
):
    parts, row_count, cols = rows_pre.shape
    own_rows = pre_first.shape[0]
    slots = row_count - own_rows
    width = parts * cols
    total = jnp.zeros((row_count, cols), jnp.float32)
    total_square = jnp.zeros((row_count, cols), jnp.float32)
    for t in range(parts):
        block = rows_pre[t].astype(jnp.float32)
        total = total + block
        total_square = total_square + block * block
    mean = jnp.sum(total, -1, keepdims=True) / width
    square = jnp.sum(total_square, -1, keepdims=True) / width
    scale = lax.rsqrt(square - mean * mean + NORM_EPS)
    for t in range(parts):
        block = (rows_pre[t].astype(jnp.float32) - mean) * scale * gains[t : t + 1]
        normed[:, t * cols : (t + 1) * cols] = block.astype(normed.dtype)
    normed_cols[...] = ((pre_first[...] - mean[slots:]) * scale[slots:] * own_gain[...]).astype(
        normed_cols.dtype
    )
    units = gate_up.shape[0] // 2
    both = f32_dot(normed[:slots], gate_up[...], ACROSS)
    routed = (jax.nn.silu(both[:, :units]) * both[:, units:]).astype(message.dtype)
    for t in range(message.shape[0]):
        message[t, :slots] = routed
    local = f32_dot(normed[slots:], local_weights[...], ACROSS)
    cut = (local.shape[1] - RIDER) // 2
    mine = jax.nn.silu(local[:, :cut]) * local[:, cut : 2 * cut]
    mine = jnp.concatenate([mine, jnp.zeros((own_rows, units // 2 - cut), jnp.float32)], 1)
    half = own_rows // 2
    packed = jnp.concatenate([mine[:half], mine[half:]], 1).astype(message.dtype)
    for t in range(message.shape[0]):
        message[t, slots:] = packed
    switch[...] = jax.nn.sigmoid(local[:, 2 * cut : 2 * cut + 1])


def hidden_units(rows_pre, gains, pre_first, own_gain, local_weights, gate_up):
    parts, row_count, cols = rows_pre.shape
    units = gate_up.shape[0] // 2
    own_rows = pre_first.shape[0]
    whole = pl.BlockSpec(memory_space=pltpu.VMEM)
    return pl.pallas_call(
        hidden_kernel,
        in_specs=[whole] * 6,
        out_specs=[whole] * 3,
        out_shape=[
            jax.ShapeDtypeStruct((parts, row_count - own_rows // 2, units), jnp.bfloat16),
            pltpu.VMEM((own_rows, cols), jnp.bfloat16),
            pltpu.VMEM((own_rows, 1), jnp.float32),
        ],
        scratch_shapes=[pltpu.VMEM((row_count, parts * cols), jnp.bfloat16)],
        name="hidden_units",
        compiler_params=pltpu.CompilerParams(vmem_limit_bytes=GRANT),
    )(*near(rows_pre, gains, pre_first, own_gain, local_weights, gate_up))


def on_device(
    tokens,
    retention_state,
    lengths,
    query_weight,
    key_weight,
    value_weight,
    gate_weight,
    out_weight,
    first_gain,
    routing,
    route_weight,
    expert_gate,
    expert_up,
    expert_down,
    shared_gate,
    shared_up,
    shared_down,
    side_gate,
    side_up,
    side_down,
    side_switch,
    second_gain,
):
    bf16 = jnp.bfloat16
    seq_rows, model_width = tokens.shape
    head_count = retention_state.shape[1]
    col_count = out_weight.shape[1]
    ep_count = lax.axis_size(EP)
    tp_count = lax.axis_size(TP)
    class_count = lax.axis_size("tp_1")
    part_count = lax.axis_size("tp_0")
    local_experts = expert_gate.shape[0]
    hidden_cols = expert_gate.shape[2]
    top_count = routing.shape[1]
    capacity = (3 * seq_rows * top_count + local_experts * ep_count - 1) // (local_experts * ep_count)
    slots = ep_count * capacity
    tp_rank = lax.axis_index(TP)
    col_start = tp_rank * col_count

    folded, new_state, own_cols = retain(
        tokens,
        retention_state,
        lengths,
        query_weight,
        key_weight,
        value_weight,
        gate_weight,
        tp_rank * head_count,
    )
    folded_all = swap(folded, TP)

    same = routing.reshape(-1)[:, None] == routing.reshape(-1)[None, :]
    row_of = jnp.arange(seq_rows * top_count, dtype=jnp.int32) // top_count
    earlier = row_of[None, :] < row_of[:, None]
    position = jnp.sum((same & earlier).astype(jnp.int32), 1).reshape(seq_rows, top_count)
    back_pitch = local_experts * capacity
    out_pitch = back_pitch + RIDER
    place = (routing % local_experts) * capacity + position
    out_ids = (routing // local_experts) * out_pitch + place
    back_ids = (routing // local_experts) * back_pitch + place
    side_cols = side_gate.shape[1]
    side_rows = side_gate.shape[0]
    core_count = lax.axis_size("core")
    wire = jnp.arange(ep_count * out_pitch, dtype=jnp.int32)[:, None]
    chosen = jnp.arange(seq_rows + side_cols, dtype=jnp.int32)[None, :]
    rider_row = (wire // out_pitch) % core_count * RIDER + wire % out_pitch - back_pitch
    table = (wire % out_pitch >= back_pitch) & (chosen == seq_rows + rider_row)
    padded = jnp.pad(out_ids, ((0, side_cols), (0, 0)), constant_values=-1)
    for k in range(top_count):
        table = table | (wire == padded[None, :, k])
    table = table.astype(bf16)
    slot_hot = (
        back_ids.T.reshape(-1)[:, None]
        == jnp.arange(ep_count * back_pitch, dtype=jnp.int32)[None, :]
    ).astype(bf16)

    side_piece = jnp.concatenate([side_gate.T, side_up.T], 1)
    outgoing, pre_first, pre_short = dispatch_rows(
        folded_all,
        jnp.repeat(out_weight.reshape(tp_count, -1, col_count), 2, 0).reshape(-1, col_count),
        table,
        side_piece,
        own_cols,
    )
    pieces = list(
        expert_pieces(
            pre_short, jnp.swapaxes(expert_gate, 1, 2), jnp.swapaxes(expert_up, 1, 2)
        )
    )
    for d in sorted(range(1, class_count), key=lambda d: -min(d, class_count - d)):
        steps = [(i, (i + d) % class_count) for i in range(class_count)]
        pieces[d] = lax.ppermute(pieces[d], "tp_1", steps)
    arrived = swap(outgoing.reshape(-1, TILE, col_count), EP).reshape(-1, col_count)

    group_slots = local_experts * GROUP * capacity
    order = jnp.arange(group_slots, dtype=jnp.int32)
    expert, source = order // (GROUP * capacity), order // capacity % GROUP
    spot = expert * capacity + order % capacity
    rider = jnp.arange(GROUP * RIDER, dtype=jnp.int32)
    came_at = jnp.concatenate(
        [source * out_pitch + spot, rider // RIDER * out_pitch + back_pitch + rider % RIDER]
    )
    regroup = (
        came_at[:, None] == jnp.arange(GROUP * out_pitch, dtype=jnp.int32)[None, :]
    ).astype(bf16)
    to_send, side_own = slot_message(
        arrived, pre_short, regroup, local_experts, slots, part_count
    )
    side_own = side_own.reshape(ep_count, RIDER, col_count)
    side_other = lax.ppermute(side_own, "core", [(0, 1), (1, 0)])
    first_core = lax.axis_index("core") == 0
    side_all = jnp.concatenate(
        [
            jnp.where(first_core, side_own, side_other),
            jnp.where(first_core, side_other, side_own),
        ],
        1,
    ).reshape(ep_count, side_cols, 2, side_rows)
    side_all = jnp.transpose(side_all, (2, 1, 0, 3)).reshape(2, side_cols, model_width)
    rows_pre = swap(to_send.reshape(tp_count, slots + seq_rows, col_count), TP)
    own_gain = lax.dynamic_slice_in_dim(first_gain, col_start, col_count, 0)
    units = class_count * hidden_cols
    shared_cols = shared_gate.shape[1]
    local_weights = jnp.concatenate(
        [
            shared_gate.T,
            side_all[0],
            shared_up.T,
            side_all[1],
            jnp.broadcast_to(side_switch[None], (RIDER, model_width)),
        ],
        0,
    )
    hidden, normed_cols, switch = hidden_units(
        rows_pre, first_gain.reshape(tp_count, col_count), pre_first, own_gain[None], local_weights, ordered(pieces)
    )

    hidden_all = swap(hidden, TP)
    goes_at = source * back_pitch + spot
    goes = (order[:, None] == goes_at[None, :]).astype(bf16)
    down = expert_down.reshape(local_experts, part_count, units, col_count)
    sent_back = return_rows(hidden_all, down, goes, ep_count // GROUP)
    returned = swap(sent_back.reshape(-1, TILE, col_count), EP)

    local_all = hidden_all[:, slots:]
    left = jnp.arange(units, dtype=jnp.int32)[None, None, :] < units // 2
    none = jnp.zeros_like(local_all)
    local_all = in_order(
        jnp.concatenate([jnp.where(left, local_all, none), jnp.where(left, none, local_all)], 1), 1
    )

    def spread(weight, first):
        count = weight.shape[0] // tp_count
        weight = jnp.pad(
            weight.reshape(tp_count, 1, count, col_count),
            ((0, 0), (0, 0), (first, units // 2 - first - count), (0, 0)),
        )
        weight = jnp.broadcast_to(weight, (tp_count, 2, units // 2, col_count))
        return weight.reshape(tp_count * units, col_count)

    shared_out = jnp.dot(
        local_all, spread(shared_down, 0), preferred_element_type=jnp.float32
    )
    side_out = jnp.dot(
        local_all, spread(side_down, shared_cols), preferred_element_type=jnp.float32
    )
    local_sum = (
        RESIDUAL_SCALE * normed_cols.astype(jnp.float32) + shared_out + switch * side_out
    )

    picked = jnp.dot(
        slot_hot, returned.reshape(-1, col_count), preferred_element_type=jnp.float32
    ).reshape(top_count, seq_rows, col_count)
    routed = jnp.sum(picked * route_weight.T[:, :, None], 0)
    pre_second = local_sum + routed
    sums = jnp.stack([jnp.sum(pre_second, -1), jnp.sum(pre_second * pre_second, -1)])
    sums, new_state = lax.optimization_barrier((sums, new_state))
    totals = jnp.sum(to_all(sums, TP), 0)
    mean_second = totals[0][:, None] / model_width
    square_second = totals[1][:, None] / model_width
    output = (
        (pre_second - mean_second)
        * lax.rsqrt(square_second - mean_second * mean_second + NORM_EPS)
        * second_gain
    ).astype(bf16)
    return (output, new_state)


def solution(mesh):
    chips = mesh.devices.reshape(mesh.shape["ep"] // 2, 2, 4, 4)
    finer = Mesh(chips, (*EP, *TP))

    return jax.shard_map(
        on_device,
        mesh=finer,
        in_specs=(
            P(EP, None),
            P(EP, TP, None, None),
            P(EP),
            P(None, TP),
            P(None, TP),
            P(None, TP),
            P(None, TP),
            P(None, TP),
            P(),
            P(EP, None),
            P(EP, None),
            P(EP, None, TP),
            P(EP, None, TP),
            P(EP, None, TP),
            P(None, TP),
            P(None, TP),
            P(None, TP),
            P(EP, TP),
            P(EP, TP),
            P(None, TP),
            P(),
            P(TP),
        ),
        out_specs=(P(EP, TP), P(EP, TP, None, None)),
        check_vma=False,
    )
```
